32 devices in a mesh: sp: 16 (over z, y, core), tp: 2 (over x).
Axes of the slice: x: 2, y: 2, z: 4, core: 2. Of those that a mesh axis runs over, the one named last changes fastest.
Arguments:
- inputs: bfloat16 [8192, 3072], P('sp', 'tp'), may hold values from -6 to 6
- w_query: bfloat16 [3072, 1536], P(None, 'tp'), may hold values from -0.109375 to 0.109375
- w_key: bfloat16 [3072, 1536], P(None, 'tp'), may hold values from -0.109375 to 0.109375
- w_value: bfloat16 [3072, 1536], P(None, 'tp'), may hold values from -0.109375 to 0.109375
- rel_bias: float32 [320, 24], P(None, 'tp'), may hold values from -5 to 254
- d_out: bfloat16 [8192, 1536], P('sp', 'tp'), may hold values from -6 to 6
Outputs:
- grad_inputs: bfloat16 [8192, 3072], P('sp', 'tp')
- grad_w_query: float32 [3072, 1536], P('sp', 'tp')
- grad_w_key: float32 [3072, 1536], P('sp', 'tp')
- grad_w_value: float32 [3072, 1536], P('sp', 'tp')
- grad_bias: float32 [320, 24], P(None, 'tp')
The draws below stay inside these ranges and needn't reach their ends.
All inputs are finite; a program needn't handle non-finite values.
Results may differ from the reference program's by a relative error of at most 0.015.
Values may be sent and summed in bfloat16 or wider, within the bound.
A program may use at most 128 MiB of HBM per device.

```python
import jax
import jax.numpy as jnp
import numpy as np
from jax import lax

D = 3072
HEADS = 24
HEAD = 64
SEG = 64
LEFT = 4
REL_MAX = 256
ATT = 1536
REL_SIZE = 320
TOKENS = 8192
N_TP = 2


def draw_rel_bias(key, part):
    base = jnp.clip(jax.random.normal(key, (REL_SIZE, HEADS), jnp.float32), -5.0, 5.0)
    return base


def spiked(drawn, rng, source, target, parts, factor):
    def block_of(position):
        return (jnp.arange(drawn.shape[position]) // (drawn.shape[position] // parts)).reshape((-1,) + (1,) * (drawn.ndim - 1 - position))

    near = jax.random.permutation(rng, parts)[block_of(target)]
    far = (block_of(target) + parts // 2) % parts
    return jnp.where((block_of(source) == near) | (block_of(source) == far), factor * drawn, drawn)


def levels(key, extent, shards, smallest, largest):
    gain = 1.0
    for axis_at, shards_of in shards:
        steps = jax.random.uniform(jax.random.fold_in(jax.random.fold_in(key, 6), axis_at), (shards_of,), jnp.float32, smallest / len(shards), largest / len(shards))
        gain = gain * jnp.repeat(jnp.exp(steps), extent[axis_at] // shards_of).reshape((-1,) + (1,) * (len(extent) - 1 - axis_at))
    return gain


def noise(own_key, dims, scale, reach, cuts=(), held_as=jnp.bfloat16):
    factor_of = levels(own_key, dims, cuts, -0.22, 0.18) if cuts else 1.0
    entries = jax.random.normal(own_key, dims, jnp.float32) * scale * factor_of
    return jnp.minimum(jnp.maximum(entries, -reach), reach).astype(held_as)


def heavy_noise(own_key, extent, scale, most, split, heavy, held_as=jnp.bfloat16):
    array = scale * jax.random.normal(own_key, extent, jnp.float32)
    if split:
        array = array * levels(own_key, extent, split, -0.22, 0.18)
    return jnp.clip(spiked(array, jax.random.fold_in(own_key, 3), *heavy), -most, most).astype(held_as)


def setup_inputs(seed: int = 0) -> dict:
    keys = jax.random.split(jax.random.key(seed), 7)
    inputs = heavy_noise(keys[0], (TOKENS, D), 1.0, 6.0, ((0, 16), (1, 2)), (0, 1, 16, 2.0))
    w_query = noise(keys[1], (D, ATT), D ** -0.5, 0.109375, ((1, 2),))
    w_key = noise(keys[2], (D, ATT), D ** -0.5, 0.109375, ((1, 2),))
    w_value = noise(keys[3], (D, ATT), D ** -0.5, 0.109375, ((1, 2),))
    rel_bias = draw_rel_bias(jax.random.fold_in(keys[6], 71), 0)
    d_out = noise(keys[5], (TOKENS, ATT), 1.0, 6.0, ((0, 16), (1, 2)))
    return dict(inputs=inputs, w_query=w_query, w_key=w_key, w_value=w_value, rel_bias=rel_bias, d_out=d_out)


def bias_table(rel_bias):
    query_row = np.arange(SEG)[:, None]
    key_row = np.arange((LEFT + 1) * SEG)[None, :]
    distance = np.clip(LEFT * SEG + query_row - key_row, 1 - SEG, REL_MAX) + SEG - 1
    picked = jnp.take(rel_bias, jnp.asarray(distance.astype(np.int32)), axis=0)
    return jnp.transpose(picked, (2, 0, 1))

def banded(source, seg_count):
    pieces = source.reshape((seg_count + LEFT, SEG) + source.shape[1:])
    return jnp.concatenate([pieces[offset_seg:offset_seg + seg_count] for offset_seg in range(LEFT + 1)], axis=1)

def unbanded(band_grads, seg_count):
    pieces = band_grads.reshape((seg_count, LEFT + 1, SEG) + band_grads.shape[2:])
    widths = ((0, 0),) * (pieces.ndim - 3)
    total = jnp.zeros((seg_count + LEFT, SEG) + band_grads.shape[2:], band_grads.dtype)
    for offset_seg in range(LEFT + 1):
        total = total + jnp.pad(pieces[:, offset_seg], ((offset_seg, LEFT - offset_seg), (0, 0)) + widths)
    return total.reshape(((seg_count + LEFT) * SEG,) + band_grads.shape[2:])

def one_head(operands):
    q_head, k_head, v_head, d_head, bias_head = operands
    seg_count = TOKENS // SEG
    score_scale = HEAD ** (-0.5)
    pad_rows = ((LEFT * SEG, 0), (0, 0))
    key_band = banded(jnp.pad(k_head, pad_rows), seg_count).astype(jnp.float32)
    value_band = banded(jnp.pad(v_head, pad_rows), seg_count).astype(jnp.float32)
    q_seg = q_head.reshape(seg_count, SEG, HEAD).astype(jnp.float32)
    d_seg = d_head.reshape(seg_count, SEG, HEAD).astype(jnp.float32)
    scores = jnp.einsum('cqd,ckd->cqk', q_seg, key_band) * score_scale + bias_head[None]
    key_pos = (jnp.arange(seg_count)[:, None] - LEFT) * SEG + jnp.arange((LEFT + 1) * SEG)[None, :]
    scores = jnp.where((key_pos >= 0)[:, None, :], scores, -jnp.inf)
    top = lax.optimization_barrier(jnp.max(scores, axis=-1, keepdims=True))
    lse = top + jnp.log(lax.optimization_barrier(jnp.sum(jnp.exp(scores - top), axis=-1, keepdims=True)))
    prob = jnp.exp(scores - lse)
    prob_low = prob.astype(jnp.bfloat16).astype(jnp.float32)
    attended = jnp.einsum('cqk,ckd->cqd', prob_low, value_band)
    delta = lax.optimization_barrier(jnp.sum(d_seg * attended, axis=-1, keepdims=True))
    grad_prob = jnp.einsum('cqd,ckd->cqk', d_seg, value_band)
    dscore = prob * (grad_prob - delta)
    dscore_low = dscore.astype(jnp.bfloat16).astype(jnp.float32)
    grad_query = jnp.einsum('cqk,ckd->cqd', dscore_low, key_band) * score_scale
    grad_kband = jnp.einsum('cqk,cqd->ckd', dscore_low, q_seg) * score_scale
    grad_vband = jnp.einsum('cqk,cqd->ckd', prob_low, d_seg)
    grad_key = unbanded(grad_kband, seg_count)[LEFT * SEG:]
    grad_value = unbanded(grad_vband, seg_count)[LEFT * SEG:]
    return (grad_query.reshape(TOKENS, HEAD).astype(jnp.bfloat16), grad_key.astype(jnp.bfloat16), grad_value.astype(jnp.bfloat16), lax.optimization_barrier(jnp.sum(dscore, axis=0)))

def reference(inputs, w_query, w_key, w_value, rel_bias, d_out):
    query = jnp.dot(inputs, w_query, preferred_element_type=jnp.float32).astype(jnp.bfloat16)
    key = jnp.dot(inputs, w_key, preferred_element_type=jnp.float32).astype(jnp.bfloat16)
    value = jnp.dot(inputs, w_value, preferred_element_type=jnp.float32).astype(jnp.bfloat16)

    def by_head(matrix):
        return matrix.reshape(TOKENS, HEADS, HEAD).transpose(1, 0, 2)

    def by_token(matrix):
        return matrix.transpose(1, 0, 2).reshape(TOKENS, HEADS * HEAD)
    bias_full, bias_back = jax.vjp(bias_table, rel_bias)
    head_q, head_k, head_v, score_sum = lax.map(one_head, (by_head(query), by_head(key), by_head(value), by_head(d_out), bias_full))
    grad_query = by_token(head_q)
    grad_key = by_token(head_k)
    grad_value = by_token(head_v)
    grad_bias = bias_back(score_sum)[0]
    contract = (((0,), (0,)), ((), ()))
    grad_w_query = lax.dot_general(inputs, grad_query, contract, preferred_element_type=jnp.float32)
    grad_w_key = lax.dot_general(inputs, grad_key, contract, preferred_element_type=jnp.float32)
    grad_w_value = lax.dot_general(inputs, grad_value, contract, preferred_element_type=jnp.float32)
    group = HEADS * HEAD // N_TP
    total = jnp.zeros((TOKENS, D), jnp.float32)
    for index in range(N_TP):
        cols = slice(index * group, (index + 1) * group)
        partial_value = jnp.dot(grad_query[:, cols], w_query[:, cols].T, preferred_element_type=jnp.float32)
        partial_value = partial_value + jnp.dot(grad_key[:, cols], w_key[:, cols].T, preferred_element_type=jnp.float32)
        partial_value = partial_value + jnp.dot(grad_value[:, cols], w_value[:, cols].T, preferred_element_type=jnp.float32)
        rounded = lax.optimization_barrier(partial_value.astype(jnp.bfloat16))
        total = total + rounded.astype(jnp.float32)
    grad_inputs = total.astype(jnp.bfloat16)
    return (grad_inputs, grad_w_query, grad_w_key, grad_w_value, grad_bias)
```

```python
import functools

import jax
import jax.numpy as jnp
from jax import lax
from jax.experimental import pallas as pl
from jax.experimental.pallas import tpu as pltpu
from jax.sharding import PartitionSpec as P

HEAD = 64
SEG = 64
LEFT = 4
REL_MAX = 256
LANES = 128
QB = 2 * SEG
HALO = LEFT * SEG
KB = HALO + QB
LINE = 512
UNSEEN = -1e30
CHUNK = 128
TILE = 256
TRIO = 3 * LANES
MESH = pl.DeviceIdType.MESH
BF = jnp.bfloat16
F32 = jnp.float32


def dot32(a, b, dims):
    return lax.dot_general(a, b, (dims, ((), ())), preferred_element_type=F32)


def exact(a, b, dims):
    return lax.dot_general(
        a, b, (dims, ((), ())), precision=lax.Precision.HIGHEST, preferred_element_type=F32
    )


def grid_of(chips):
    depth = 1
    while depth * depth < chips:
        depth *= 2
    return depth, chips // depth


def aligned(index, size):
    return pl.ds(pl.multiple_of(index * size, size), size)


def bias_index(apart):
    return jnp.clip(HALO + apart, 1 - SEG, REL_MAX) + SEG - 1


def step_body(
    sizes,
    x_ref, wq_ref, wk_ref, wv_ref, rel_ref, d_ref,
    gi_ref, dwq_ref, dwk_ref, dwv_ref, gb_ref,
    xw, wcat, xt, xg, zacc, q_s, k_ext, v_ext, d_s, lines, dline, bias, bias_sum, kacc, vacc,
    halo_s, halo_r, dall, rr, rl, pxs, pxr, bslot, brecv,
    w_sem, d_sem, x_sem, xs_sem, xr_sem, gs_sem, gr_sem, gl_sem, ks_sem, kr_sem, hs_sem, hr_sem,
    ys_sem, yr_sem, cs_sem, cr_sem, rs_sem, rv_sem, ls_sem, lv_sem, bs_sem, br_sem, ps_sem, pr_sem,
):
    seq, tps = sizes
    deep, wide = grid_of(seq // 2)
    rows, dloc = x_ref.shape
    pairs = wq_ref.shape[1] // LANES
    ext = HALO + rows
    blocks = rows // QB
    feat = dloc * tps // seq
    group = 2 * wide
    sp = lax.axis_index("sp")
    tp = lax.axis_index("tp")
    core = lax.rem(sp, 2)
    chip = lax.div(sp, 2)
    y = lax.rem(chip, wide)
    z = lax.div(chip, wide)
    mine = y * 2 + core

    def at(zi, yi, ci):
        return ((zi * wide + yi) * 2 + ci, tp)

    def mod(a, n):
        return lax.rem(a + n, n)

    mate = at(z, y, 1 - core)
    ahead, behind = (sp + 1, tp), (sp - 1, tp)
    has_ahead, has_behind = sp + 1 < seq, sp > 0

    greeted = [(sp, mod(tp + k, tps)) for k in range(1, tps)]
    greeted += [(mod(sp + 1, seq), tp), (mod(sp - 1, seq), tp)]
    greeted += [at(z, mod(y + j, wide), mod(core + i, 2)) for j in range(wide) for i in range(2) if i + j]
    greeted += [at(mod(z + 1, deep), y, core), at(mod(z - 1, deep), y, core)]
    steps = seq.bit_length() - 1
    greeted += [(jnp.bitwise_xor(sp, 1 << k), tp) for k in range(steps)]
    barrier = pltpu.get_barrier_semaphore()
    for other in greeted:
        pl.semaphore_signal(barrier, inc=1, device_id=other, device_id_type=MESH)
    pl.semaphore_wait(barrier, len(greeted))

    def remote(src, dst, send, recv, device):
        return pltpu.make_async_remote_copy(
            src_ref=src, dst_ref=dst, send_sem=send, recv_sem=recv,
            device_id=device, device_id_type=MESH,
        )

    chunks = rows // CHUNK
    first = (rows - HALO) // CHUNK
    order = list(range(first, chunks)) + list(range(first))

    def x_copy(k, r):
        part = slice(r * CHUNK, (r + 1) * CHUNK)
        return remote(
            x_ref.at[part, :], xw.at[part, aligned(tp, dloc)],
            xs_sem.at[k - 1, r], xr_sem.at[k - 1, r], (sp, mod(tp + k, tps)),
        )

    for r in order:
        for k in range(1, tps):
            x_copy(k, r).start()
    own_x = pltpu.make_async_copy(x_ref, xw.at[:, aligned(tp, dloc)], x_sem)
    own_x.start()
    for p in range(pairs):
        for j, w_ref in enumerate((wq_ref, wk_ref, wv_ref)):
            pltpu.make_async_copy(
                w_ref.at[:, p * LANES : (p + 1) * LANES],
                wcat.at[:, p * TRIO + j * LANES : p * TRIO + (j + 1) * LANES], w_sem,
            ).start()
    for p in range(pairs):
        pltpu.make_async_copy(
            d_ref.at[:, p * LANES : (p + 1) * LANES], d_s.at[p], d_sem
        ).start()
    own_x.wait()

    def turn(t, r):
        part = slice(r * CHUNK, (r + 1) * CHUNK)

        @pl.loop(0, dloc // TILE)
        def _(f):
            cols = aligned(t * (dloc // TILE) + f, TILE)
            xt[cols, part] = xw[part, cols].T

    zparts = deep // tps

    def share(t, low, high):
        for j in range(wide):
            for i in range(2):
                for q in range(zparts):
                    zb = t * zparts + q
                    y2, c2 = mod(y + j, wide), mod(core + i, 2)
                    src = xt.at[aligned((zb * wide + y2) * 2 + c2, feat), low:high]
                    cols = pl.ds(pl.multiple_of(mine * rows + low, CHUNK), high - low)
                    dst = xg.at[aligned(zb, feat), cols]
                    if i + j:
                        remote(src, dst, gs_sem, gr_sem, at(z, y2, c2)).start()
                    else:
                        pltpu.make_async_copy(src, dst, gl_sem).start()

    for r in range(chunks):
        turn(tp, r)
    share(tp, 0, rows)

    pltpu.make_async_copy(wcat, wcat, w_sem).wait()

    @pl.loop(0, pairs)
    def _(p):
        zacc[p, :rows, :] = dot32(
            xw[:, aligned(tp, dloc)], wcat[aligned(tp, dloc), aligned(p, TRIO)], ((1,), (0,))
        )

    @pl.when(sp == 0)
    def _():
        k_ext[:, :HALO, :] = jnp.zeros((pairs, HALO, LANES), BF)
        v_ext[:, :HALO, :] = jnp.zeros((pairs, HALO, LANES), BF)

    spot = lax.broadcasted_iota(jnp.int32, (rel_ref.shape[1], LINE), 1)
    entry = lax.broadcasted_iota(jnp.int32, (rel_ref.shape[1], LINE), 0)
    apart = jnp.where(spot < QB, spot, spot - LINE)
    picked = exact(rel_ref[...], jnp.where(bias_index(apart) == entry, 1.0, 0.0), ((1,), (0,)))
    for n in range(2 * pairs):
        lines[n] = picked[n : n + 1, :]

    def halo_copy(ref, n):
        return remote(
            ref.at[:, rows : rows + HALO, :], ref.at[:, :HALO, :],
            ks_sem.at[n], kr_sem.at[n], ahead,
        )

    for n, r in enumerate(order):
        part = slice(r * CHUNK, (r + 1) * CHUNK)
        for k in range(1, tps):
            x_copy(k, r).wait_recv()

        @pl.loop(0, pairs)
        def _(p):
            total = zacc[p, part, :]
            for k in range(1, tps):
                t = mod(tp - k, tps)
                total = total + dot32(
                    xw[part, aligned(t, dloc)], wcat[aligned(t, dloc), aligned(p, TRIO)],
                    ((1,), (0,)),
                )
            low = total.astype(BF)
            q_s[p, part, :] = low[:, :LANES]
            k_ext[p, HALO + r * CHUNK : HALO + (r + 1) * CHUNK, :] = low[:, LANES : 2 * LANES]
            v_ext[p, HALO + r * CHUNK : HALO + (r + 1) * CHUNK, :] = low[:, 2 * LANES :]

        if n == chunks - first - 1:
            @pl.when(has_ahead)
            def _():
                halo_copy(k_ext, 0).start()
                halo_copy(v_ext, 1).start()

        for k in range(1, tps):
            t = mod(tp - k, tps)
            turn(t, r)
            share(t, r * CHUNK, (r + 1) * CHUNK)

    pltpu.make_async_copy(d_s, d_s, d_sem).wait()

    @pl.when(has_behind)
    def _():
        halo_copy(k_ext, 0).wait_recv()
        halo_copy(v_ext, 1).wait_recv()

    key_row = lax.broadcasted_iota(jnp.int32, (KB, QB), 0)
    query_row = lax.broadcasted_iota(jnp.int32, (KB, QB), 1)
    lane = lax.broadcasted_iota(jnp.int32, (QB, LANES), 1)
    scale = HEAD ** (-0.5)
    zero = jnp.zeros((QB, LANES), BF)
    own_rows = aligned(mine, rows)

    def stacked(part):
        return jnp.concatenate(
            [jnp.where(lane < HEAD, part, zero), jnp.where(lane < HEAD, zero, part)], axis=0
        )

    def grad_halo(p):
        return remote(halo_s.at[p], halo_r.at[p], hs_sem.at[p], hr_sem.at[p], behind)

    def attend(p):
        slot = lax.rem(p, 2)
        offset = key_row - jnp.where(query_row < SEG, 0, SEG)
        seen = (offset >= 0) & (offset < HALO + SEG)
        for half in range(2):
            line = jnp.broadcast_to(lines[2 * p + half], (KB, LINE))
            skewed = pltpu.roll(line, 0, 1, stride=1, stride_axis=0)[:, :QB]
            bias[:, half * QB : (half + 1) * QB] = jnp.where(seen, skewed, UNSEEN)
        kacc[slot] = jnp.zeros((ext, LANES), F32)
        vacc[slot] = jnp.zeros((ext, LANES), F32)
        bias_sum[...] = jnp.zeros_like(bias_sum)
        for block in range(blocks):
            keys = slice(block * QB, block * QB + KB)
            part = slice(block * QB, (block + 1) * QB)
            q2 = stacked(q_s[p, part, :] * BF(scale))
            d2 = stacked(d_s[p, part, :])
            k = k_ext[p, keys, :]
            v = v_ext[p, keys, :]
            score = dot32(k, q2, ((1,), (1,))) + bias[...]
            if block * QB < HALO:
                row = lax.broadcasted_iota(jnp.int32, (KB, 1), 0) + block * QB
                score = score + jnp.where((row < HALO) & (sp == 0), UNSEEN, 0.0)
            top = jnp.max(score, axis=0, keepdims=True)
            power = jnp.exp(score - top)
            prob = power * (1.0 / jnp.sum(power, axis=0, keepdims=True))
            prob_low = prob.astype(BF)
            grad_prob = dot32(v, d2, ((1,), (1,)))
            delta = jnp.sum(prob_low.astype(F32) * grad_prob, axis=0, keepdims=True)
            dscore = prob * (grad_prob - delta)
            bias_sum[...] += dscore
            dscore_low = dscore.astype(BF)
            vacc[slot, keys, :] += dot32(prob_low, d2, ((1,), (0,)))
            kacc[slot, keys, :] += dot32(dscore_low, q2, ((1,), (0,)))
            dq_t = dot32(k, dscore_low, ((0,), (0,)))
            dq_t = jnp.concatenate([dq_t[:HEAD, :QB], dq_t[HEAD:, QB:]], axis=0)
            dq = (dq_t.T * scale).astype(BF)
            xw[part, aligned(p * 3, LANES)] = dq
            dall[p, pl.ds(pl.multiple_of(mine * rows + block * QB, QB), QB), :LANES] = dq
        halo_s[p, 0] = kacc[slot, :HALO, :].astype(BF)
        halo_s[p, 1] = vacc[slot, :HALO, :].astype(BF)

        @pl.when(has_behind)
        def _():
            grad_halo(p).start()

        flip_row = lax.broadcasted_iota(jnp.int32, (KB, KB), 0)
        flip_col = lax.broadcasted_iota(jnp.int32, (KB, KB), 1)
        flip = jnp.where(flip_row + flip_col == KB - 1, 1.0, 0.0)
        flipped = exact(flip, bias_sum[...], ((1,), (0,)))
        for half in range(2):
            part = flipped[:, half * QB : (half + 1) * QB]
            spread = jnp.concatenate([part, jnp.zeros((KB, LINE - QB), F32)], axis=1)
            skewed = pltpu.roll(spread, 0, 1, stride=1, stride_axis=0)
            dline[2 * p + half] = jnp.sum(skewed, axis=0, keepdims=True)

    def to_wide(p, k):
        view = dall.at[p, own_rows, :]
        return remote(
            view, view, ys_sem.at[p, k - 1], yr_sem.at[p, k - 1], at(z, mod(y + k, wide), core)
        )

    def to_mate(p, k):
        owner = aligned(mod(y - k, wide) * 2 + core, rows)
        view = dall.at[p, owner, :]
        return remote(view, view, cs_sem.at[p, k], cr_sem.at[p, k], mate)

    def settle(p):
        slot = lax.rem(p, 2)

        @pl.when(has_ahead)
        def _():
            grad_halo(p).wait_recv()
            kacc[slot, rows:, :] += halo_r[p, 0].astype(F32)
            vacc[slot, rows:, :] += halo_r[p, 1].astype(F32)

        for j, total in ((1, kacc), (2, vacc)):
            low = total[slot, HALO:, :].astype(BF)
            xw[:, aligned(p * 3 + j, LANES)] = low
            dall[p, own_rows, j * LANES : (j + 1) * LANES] = low
        for k in range(1, wide):
            to_wide(p, k).start()
        to_mate(p, 0).start()

    def forward(p):
        for k in range(1, wide):
            to_wide(p, k).wait_recv()
            to_mate(p, k).start()

    def block_of(b):
        return slice(b * feat, (b + 1) * feat)

    def to_right(p, b):
        return remote(
            rr.at[p, b], rr.at[p, b], rs_sem.at[p, b], rv_sem.at[p, b], at(z + 1, y, core)
        )

    def to_left(p, b):
        return remote(
            rl.at[p, b], rl.at[p, b], ls_sem.at[p, b], lv_sem.at[p, b], at(z - 1, y, core)
        )

    def hop(p, h):
        @pl.when(z == h)
        def _():
            for b in range(deep - 1, h, -1):
                total = zacc[p, block_of(b), :]
                if h:
                    to_right(p, b).wait_recv()
                    total = total + rr[p, b].astype(F32)
                rr[p, b] = total.astype(BF)
                to_right(p, b).start()

        @pl.when(z == deep - 1 - h)
        def _():
            for b in range(0, deep - 1 - h):
                total = zacc[p, block_of(b), :]
                if h:
                    to_left(p, b).wait_recv()
                    total = total + rl[p, b].astype(F32)
                rl[p, b] = total.astype(BF)
                to_left(p, b).start()

    def product(p):
        for k in range(wide):
            to_mate(p, k).wait_recv()

        @pl.when(p == 0)
        def _():
            some = xg.at[:, : (group - 1) * rows]
            pltpu.make_async_copy(some, some, gr_sem).wait()
            some = xg.at[:, :rows]
            pltpu.make_async_copy(some, some, gl_sem).wait()

        zacc[p, : deep * feat, :] = dot32(xg[...], dall[p], ((1,), (0,)))
        hop(p, 0)

    def finish(p):
        me = aligned(z, feat)

        @pl.when(z > 0)
        def _():
            to_right(p, z).wait_recv()
            zacc[p, me, :] += rr[p, z].astype(F32)

        @pl.when(z < deep - 1)
        def _():
            to_left(p, z).wait_recv()
            zacc[p, me, :] += rl[p, z].astype(F32)

        total = zacc[p, me, :]
        for j, ref in enumerate((dwq_ref, dwk_ref, dwv_ref)):
            ref[:, aligned(p, LANES)] = total[:, j * LANES : (j + 1) * LANES]

    def bias_copy(k):
        return remote(
            bslot.at[k], brecv.at[k], bs_sem.at[k], br_sem.at[k],
            (jnp.bitwise_xor(sp, 1 << k), tp),
        )

    def bias_step(k):
        if k:
            bias_copy(k - 1).wait_recv()
            bslot[k] = bslot[k - 1] + brecv[k - 1]
        else:
            bslot[0] = jnp.concatenate([dline[n] for n in range(2 * pairs)], axis=0)
        if k < steps:
            bias_copy(k).start()

    tiles = dloc // TILE
    away = (tps - 1) * tiles

    def px_copy(j):
        return remote(
            pxs.at[j], pxr.at[j], ps_sem, pr_sem, (sp, mod(tp + 1 + lax.div(j, tiles), tps))
        )

    def input_tile(j):
        place = mod(tp + 1 + lax.div(j, tiles), tps) * tiles + lax.rem(j, tiles)
        low = dot32(
            xw[:, : pairs * TRIO], wcat[aligned(place, TILE), :], ((1,), (1,))
        ).astype(BF)

        @pl.when(j < away)
        def _():
            pxs[j] = low
            px_copy(j).start()

        @pl.when(j >= away)
        def _():
            gi_ref[:, aligned(j - away, TILE)] = low

    hops = deep - 2
    lag_end = 5 + hops
    rounds = pairs + lag_end + 1
    late = rounds - (pairs + 1)
    per = -(-tps * tiles // late)

    def staged(i, lag, stage):
        p = i - lag

        @pl.when((p >= 0) & (p < pairs))
        def _():
            stage(p)

    @pl.loop(0, rounds)
    def _(i):
        staged(i, 0, attend)
        staged(i, 1, settle)
        staged(i, 3, forward)
        staged(i, 4, product)
        for h in range(1, hops + 1):
            staged(i, 4 + h, functools.partial(hop, h=h))
        staged(i, lag_end, finish)
        for k in range(steps + 1):
            @pl.when(i == pairs + k)
            def _():
                bias_step(k)

        @pl.when(i > pairs)
        def _():
            @pl.loop(0, per)
            def _(n):
                j = (i - pairs - 1) * per + n

                @pl.when(j < tps * tiles)
                def _():
                    input_tile(j)

    spot = lax.broadcasted_iota(jnp.int32, (rel_ref.shape[1], LINE), 1)
    back = bias_index(spot - (KB - 1))
    entry = lax.broadcasted_iota(jnp.int32, (rel_ref.shape[1], LINE), 0)
    gb_ref[...] = exact(bslot[steps], jnp.where(back == entry, 1.0, 0.0), ((1,), (1,)))

    pltpu.make_async_copy(pxr, pxr, pr_sem).wait()
    for n in range(tiles):
        cols = slice(n * TILE, (n + 1) * TILE)
        total = gi_ref[:, cols].astype(F32)
        for k in range(1, tps):
            total = total + pxr[(k - 1) * tiles + n].astype(F32)
        gi_ref[:, cols] = total.astype(BF)

    pltpu.make_async_copy(pxs, pxs, ps_sem).wait()
    for r in order:
        for k in range(1, tps):
            x_copy(k, r).wait_send()
    some = xg.at[:, : (group - 1) * rows]
    pltpu.make_async_copy(some, some, gs_sem).wait()

    @pl.when(has_ahead)
    def _():
        halo_copy(k_ext, 0).wait_send()
        halo_copy(v_ext, 1).wait_send()

    for k in range(steps):
        bias_copy(k).wait_send()

    @pl.loop(0, pairs)
    def _(p):
        @pl.when(has_behind)
        def _():
            grad_halo(p).wait_send()

        for k in range(1, wide):
            to_wide(p, k).wait_send()
        for k in range(wide):
            to_mate(p, k).wait_send()
        for b in range(deep):
            @pl.when(z < b)
            def _():
                to_right(p, b).wait_send()

            @pl.when(z > b)
            def _():
                to_left(p, b).wait_send()


def local(sizes, inputs, w_query, w_key, w_value, rel_bias, d_out):
    seq, tps = sizes
    deep, wide = grid_of(seq // 2)
    rows, dloc = inputs.shape
    full, width = w_query.shape
    pairs = width // LANES
    ext = HALO + rows
    feat = full // seq
    group = 2 * wide
    tiles = dloc // TILE
    steps = seq.bit_length() - 1
    chunks = rows // CHUNK
    heads = rel_bias.shape[1]
    sds = jax.ShapeDtypeStruct
    vm = pltpu.VMEM
    dma = pltpu.SemaphoreType.DMA
    hbm = pl.BlockSpec(memory_space=pl.ANY)
    on_chip = pl.BlockSpec(memory_space=pltpu.VMEM)
    out = pl.pallas_call(
        functools.partial(step_body, sizes),
        in_specs=[hbm, hbm, hbm, hbm, on_chip, hbm],
        out_specs=[on_chip] * 5,
        out_shape=[
            sds((rows, dloc), BF),
            sds((feat, width), F32), sds((feat, width), F32), sds((feat, width), F32),
            sds((heads, rel_bias.shape[0]), F32),
        ],
        scratch_shapes=[
            vm((rows, full), BF),
            vm((full, pairs * TRIO), BF),
            vm((full, rows), BF),
            vm((deep * feat, group * rows), BF),
            vm((pairs, max(deep * feat, rows), TRIO), F32),
            vm((pairs, rows, LANES), BF),
            vm((pairs, ext, LANES), BF),
            vm((pairs, ext, LANES), BF),
            vm((pairs, rows, LANES), BF),
            vm((2 * pairs, 1, LINE), F32),
            vm((2 * pairs, 1, LINE), F32),
            vm((KB, 2 * QB), F32),
            vm((KB, 2 * QB), F32),
            vm((2, ext, LANES), F32),
            vm((2, ext, LANES), F32),
            vm((pairs, 2, HALO, LANES), BF),
            vm((pairs, 2, HALO, LANES), BF),
            vm((pairs, group * rows, TRIO), BF),
            vm((pairs, deep, feat, TRIO), BF),
            vm((pairs, deep, feat, TRIO), BF),
            vm(((tps - 1) * tiles, rows, TILE), BF),
            vm(((tps - 1) * tiles, rows, TILE), BF),
            vm((steps + 1, 2 * pairs, LINE), F32),
            vm((steps, 2 * pairs, LINE), F32),
            dma(()), dma(()), dma(()),
            dma((tps - 1, chunks)), dma((tps - 1, chunks)),
            dma(()), dma(()), dma(()),
            dma((2,)), dma((2,)),
            dma((pairs,)), dma((pairs,)),
            dma((pairs, wide - 1)), dma((pairs, wide - 1)),
            dma((pairs, wide)), dma((pairs, wide)),
            dma((pairs, deep)), dma((pairs, deep)),
            dma((pairs, deep)), dma((pairs, deep)),
            dma((steps,)), dma((steps,)),
            dma(()), dma(()),
        ],
        compiler_params=pltpu.CompilerParams(
            collective_id=0, has_side_effects=True, vmem_limit_bytes=67043328
        ),
        name="whole_step",
    )(inputs, w_query, w_key, w_value, rel_bias.T, d_out)
    return out[0], out[1], out[2], out[3], out[4].T


def solution(mesh):
    placed = (
        P("sp", "tp"),
        P(None, "tp"),
        P(None, "tp"),
        P(None, "tp"),
        P(None, "tp"),
        P("sp", "tp"),
    )
    sizes = (mesh.shape["sp"], mesh.shape["tp"])
    return jax.shard_map(
        functools.partial(local, sizes),
        mesh=mesh,
        in_specs=placed,
        out_specs=(P("sp", "tp"), P("sp", "tp"), P("sp", "tp"), P("sp", "tp"), P(None, "tp")),
        check_vma=False,
    )
```

```python
import functools

import jax
import jax.numpy as jnp
from jax import lax
from jax.experimental import pallas as pl
from jax.experimental.pallas import tpu as pltpu
from jax.sharding import PartitionSpec as P

HEAD = 64
SEG = 64
LEFT = 4
REL_MAX = 256
LANES = 128
QB = 2 * SEG
HALO = LEFT * SEG
KB = HALO + QB
LINE = 512
UNSEEN = -1e30
CHUNK = 128
TILE = 256
TRIO = 3 * LANES
MESH = pl.DeviceIdType.MESH
BF = jnp.bfloat16
F32 = jnp.float32


def dot32(a, b, dims):
    return lax.dot_general(a, b, (dims, ((), ())), preferred_element_type=F32)


def exact(a, b, dims):
    return lax.dot_general(
        a, b, (dims, ((), ())), precision=lax.Precision.HIGHEST, preferred_element_type=F32
    )


def grid_of(chips):
    depth = 1
    while depth * depth < chips:
        depth *= 2
    return depth, chips // depth


def aligned(index, size):
    return pl.ds(pl.multiple_of(index * size, size), size)


def bias_index(apart):
    return jnp.clip(HALO + apart, 1 - SEG, REL_MAX) + SEG - 1


def step_body(
    sizes,
    x_ref, wq_ref, wk_ref, wv_ref, rel_ref, d_ref,
    gi_ref, dwq_ref, dwk_ref, dwv_ref, gb_ref,
    xw, wcat, xt, xg, zacc, q_s, k_ext, v_ext, d_s, lines, dline, bias, bias_sum, kacc, vacc,
    halo_s, halo_r, all_q, all_kv, right_q, right_kv, left_q, left_kv, pxs, pxr, near, far,
    w_sem, d_sem, x_sem, xs_sem, xr_sem, gs_sem, gr_sem, gl_sem, ks_sem, kr_sem, hs_sem, hr_sem,
    ys_sem, yr_sem, cs_sem, cr_sem, rs_sem, rv_sem, ls_sem, lv_sem, bs_sem, br_sem, ps_sem, pr_sem,
):
    alls, rights, lefts = (all_q, all_kv), (right_q, right_kv), (left_q, left_kv)
    lanes = (slice(0, LANES), slice(LANES, TRIO))
    seq, tps = sizes
    deep, wide = grid_of(seq // 2)
    rows, dloc = x_ref.shape
    pairs = wq_ref.shape[1] // LANES
    ext = HALO + rows
    blocks = rows // QB
    feat = dloc * tps // seq
    group = 2 * wide
    sp = lax.axis_index("sp")
    tp = lax.axis_index("tp")
    core = lax.rem(sp, 2)
    chip = lax.div(sp, 2)
    y = lax.rem(chip, wide)
    z = lax.div(chip, wide)
    mine = y * 2 + core

    def at(zi, yi, ci):
        return ((zi * wide + yi) * 2 + ci, tp)

    def mod(a, n):
        return lax.rem(a + n, n)

    mate = at(z, y, 1 - core)
    ahead, behind = (sp + 1, tp), (sp - 1, tp)
    has_ahead, has_behind = sp + 1 < seq, sp > 0

    greeted = [(sp, mod(tp + k, tps)) for k in range(1, tps)]
    greeted += [(mod(sp + 1, seq), tp), (mod(sp - 1, seq), tp)]
    greeted += [at(z, mod(y + j, wide), mod(core + i, 2)) for j in range(wide) for i in range(2) if i + j]
    greeted += [at(mod(z + k, deep), y, core) for k in range(1, deep)]
    barrier = pltpu.get_barrier_semaphore()
    for other in greeted:
        pl.semaphore_signal(barrier, inc=1, device_id=other, device_id_type=MESH)

    own_x = pltpu.make_async_copy(x_ref, xw.at[:, aligned(tp, dloc)], x_sem)
    own_x.start()
    for p in range(pairs):
        for j, w_ref in enumerate((wq_ref, wk_ref, wv_ref)):
            pltpu.make_async_copy(
                w_ref.at[:, p * LANES : (p + 1) * LANES],
                wcat.at[:, p * TRIO + j * LANES : p * TRIO + (j + 1) * LANES], w_sem,
            ).start()
    for p in range(pairs):
        pltpu.make_async_copy(
            d_ref.at[:, p * LANES : (p + 1) * LANES], d_s.at[p], d_sem
        ).start()
    pl.semaphore_wait(barrier, len(greeted))

    def remote(src, dst, send, recv, device):
        return pltpu.make_async_remote_copy(
            src_ref=src, dst_ref=dst, send_sem=send, recv_sem=recv,
            device_id=device, device_id_type=MESH,
        )

    chunks = rows // CHUNK
    first = (rows - HALO) // CHUNK
    order = list(range(first, chunks)) + list(range(first))

    def x_copy(k, r):
        part = slice(r * CHUNK, (r + 1) * CHUNK)
        return remote(
            x_ref.at[part, :], xw.at[part, aligned(tp, dloc)],
            xs_sem.at[k - 1, r], xr_sem.at[k - 1, r], (sp, mod(tp + k, tps)),
        )

    for r in order:
        for k in range(1, tps):
            x_copy(k, r).start()
    own_x.wait()

    def turn(t, r):
        part = slice(r * CHUNK, (r + 1) * CHUNK)

        @pl.loop(0, dloc // TILE)
        def _(f):
            cols = aligned(t * (dloc // TILE) + f, TILE)
            xt[cols, part] = xw[part, cols].T

    zparts = deep // tps

    def share(t, low, high, own):
        for j in range(wide):
            for i in range(2):
                for q in range(zparts):
                    zb = t * zparts + q
                    y2, c2 = mod(y + j, wide), mod(core + i, 2)
                    src = xt.at[aligned((zb * wide + y2) * 2 + c2, feat), low:high]
                    cols = pl.ds(pl.multiple_of(mine * rows + low, CHUNK), high - low)
                    dst = xg.at[aligned(zb, feat), cols]
                    if i + j:
                        remote(src, dst, gs_sem.at[own], gr_sem.at[own], at(z, y2, c2)).start()
                    else:
                        pltpu.make_async_copy(src, dst, gl_sem.at[own]).start()

    for r in range(chunks):
        turn(tp, r)
        share(tp, r * CHUNK, (r + 1) * CHUNK, 0)

    pltpu.make_async_copy(wcat, wcat, w_sem).wait()

    @pl.loop(0, pairs)
    def _(p):
        zacc[p, :rows, :] = dot32(
            xw[:, aligned(tp, dloc)], wcat[aligned(tp, dloc), aligned(p, TRIO)], ((1,), (0,))
        )

    @pl.when(sp == 0)
    def _():
        k_ext[:, :HALO, :] = jnp.zeros((pairs, HALO, LANES), BF)
        v_ext[:, :HALO, :] = jnp.zeros((pairs, HALO, LANES), BF)

    spot = lax.broadcasted_iota(jnp.int32, (rel_ref.shape[1], LINE), 1)
    entry = lax.broadcasted_iota(jnp.int32, (rel_ref.shape[1], LINE), 0)
    apart = jnp.where(spot < QB, spot, spot - LINE)
    picked = exact(rel_ref[...], jnp.where(bias_index(apart) == entry, 1.0, 0.0), ((1,), (0,)))
    for n in range(2 * pairs):
        lines[n] = picked[n : n + 1, :]

    def halo_copy(ref, n):
        return remote(
            ref.at[:, rows : rows + HALO, :], ref.at[:, :HALO, :],
            ks_sem.at[n], kr_sem.at[n], ahead,
        )

    def cross_copy(k, g):
        r = order[-1]
        view = xg.at[
            aligned(tp, zparts * feat), g * rows + r * CHUNK : g * rows + (r + 1) * CHUNK
        ]
        return remote(view, view, gs_sem.at[2], gr_sem.at[2], (sp, mod(tp + k, tps)))

    early = chunks - first - 1
    for n, r in enumerate(order):
        part = slice(r * CHUNK, (r + 1) * CHUNK)
        for k in range(1, tps):
            x_copy(k, r).wait_recv()

        if n == chunks - 1:
            some = xg.at[: zparts * feat, : (group - 1) * rows]
            pltpu.make_async_copy(some, some, gr_sem.at[0]).wait()
            some = xg.at[: zparts * feat, :rows]
            pltpu.make_async_copy(some, some, gl_sem.at[0]).wait()
            for k in range(1, tps):
                for g in range(group):
                    cross_copy(k, g).start()

        @pl.loop(0, pairs)
        def _(p):
            total = zacc[p, part, :]
            for k in range(1, tps):
                t = mod(tp - k, tps)
                total = total + dot32(
                    xw[part, aligned(t, dloc)], wcat[aligned(t, dloc), aligned(p, TRIO)],
                    ((1,), (0,)),
                )
            low = total.astype(BF)
            q_s[p, part, :] = low[:, :LANES]
            k_ext[p, HALO + r * CHUNK : HALO + (r + 1) * CHUNK, :] = low[:, LANES : 2 * LANES]
            v_ext[p, HALO + r * CHUNK : HALO + (r + 1) * CHUNK, :] = low[:, 2 * LANES :]

        if n == early:
            @pl.when(has_ahead)
            def _():
                halo_copy(k_ext, 0).start()
                halo_copy(v_ext, 1).start()

        if n < chunks - 1:
            for k in range(1, tps):
                t = mod(tp - k, tps)
                turn(t, r)
                if n > early:
                    for done in order[: n + 1] if n == early + 1 else [r]:
                        share(t, done * CHUNK, (done + 1) * CHUNK, 1)

    pltpu.make_async_copy(d_s, d_s, d_sem).wait()

    @pl.when(has_behind)
    def _():
        halo_copy(k_ext, 0).wait_recv()
        halo_copy(v_ext, 1).wait_recv()

    key_row = lax.broadcasted_iota(jnp.int32, (KB, QB), 0)
    query_row = lax.broadcasted_iota(jnp.int32, (KB, QB), 1)
    lane = lax.broadcasted_iota(jnp.int32, (QB, LANES), 1)
    scale = HEAD ** (-0.5)
    zero = jnp.zeros((QB, LANES), BF)
    own_rows = aligned(mine, rows)

    def stacked(part):
        return jnp.concatenate(
            [jnp.where(lane < HEAD, part, zero), jnp.where(lane < HEAD, zero, part)], axis=0
        )

    def grad_halo(p):
        return remote(halo_s.at[p], halo_r.at[p], hs_sem.at[p], hr_sem.at[p], behind)

    def to_wide(p, m, k):
        view = alls[m].at[p, own_rows, :]
        return remote(
            view, view, ys_sem.at[m, p, k - 1], yr_sem.at[m, p, k - 1],
            at(z, mod(y + k, wide), core),
        )

    def to_mate(p, m, k):
        owner = aligned(mod(y - k, wide) * 2 + core, rows)
        view = alls[m].at[p, owner, :]
        return remote(view, view, cs_sem.at[m, p, k], cr_sem.at[m, p, k], mate)

    def spread_out(p, m):
        for k in range(1, wide):
            to_wide(p, m, k).start()
        to_mate(p, m, 0).start()

    def attend(p):
        slot = lax.rem(p, 2)
        offset = key_row - jnp.where(query_row < SEG, 0, SEG)
        seen = (offset >= 0) & (offset < HALO + SEG)
        for half in range(2):
            line = jnp.broadcast_to(lines[2 * p + half], (KB, LINE))
            skewed = pltpu.roll(line, 0, 1, stride=1, stride_axis=0)[:, :QB]
            bias[:, half * QB : (half + 1) * QB] = jnp.where(seen, skewed, UNSEEN)
        kacc[slot] = jnp.zeros((ext, LANES), F32)
        vacc[slot] = jnp.zeros((ext, LANES), F32)
        bias_sum[...] = jnp.zeros_like(bias_sum)
        for block in range(blocks):
            keys = slice(block * QB, block * QB + KB)
            part = slice(block * QB, (block + 1) * QB)
            q2 = stacked(q_s[p, part, :] * BF(scale))
            d2 = stacked(d_s[p, part, :])
            k = k_ext[p, keys, :]
            v = v_ext[p, keys, :]
            score = dot32(k, q2, ((1,), (1,))) + bias[...]
            if block * QB < HALO:
                row = lax.broadcasted_iota(jnp.int32, (KB, 1), 0) + block * QB
                score = score + jnp.where((row < HALO) & (sp == 0), UNSEEN, 0.0)
            top = jnp.max(score, axis=0, keepdims=True)
            power = jnp.exp(score - top)
            prob = power * (1.0 / jnp.sum(power, axis=0, keepdims=True))
            prob_low = prob.astype(BF)
            grad_prob = dot32(v, d2, ((1,), (1,)))
            delta = jnp.sum(prob_low.astype(F32) * grad_prob, axis=0, keepdims=True)
            dscore = prob * (grad_prob - delta)
            bias_sum[...] += dscore
            dscore_low = dscore.astype(BF)
            vacc[slot, keys, :] += dot32(prob_low, d2, ((1,), (0,)))
            kacc[slot, keys, :] += dot32(dscore_low, q2, ((1,), (0,)))
            dq_t = dot32(k, dscore_low, ((0,), (0,)))
            dq_t = jnp.concatenate([dq_t[:HEAD, :QB], dq_t[HEAD:, QB:]], axis=0)
            dq = (dq_t.T * scale).astype(BF)
            xw[part, aligned(p * 3, LANES)] = dq
            all_q[p, pl.ds(pl.multiple_of(mine * rows + block * QB, QB), QB), :] = dq
            if block == HALO // QB - 1:
                halo_s[p, 0] = kacc[slot, :HALO, :].astype(BF)
                halo_s[p, 1] = vacc[slot, :HALO, :].astype(BF)

                @pl.when(has_behind)
                def _():
                    grad_halo(p).start()

        flip_row = lax.broadcasted_iota(jnp.int32, (KB, KB), 0)
        flip_col = lax.broadcasted_iota(jnp.int32, (KB, KB), 1)
        flip = jnp.where(flip_row + flip_col == KB - 1, 1.0, 0.0)
        flipped = exact(flip, bias_sum[...], ((1,), (0,)))
        for half in range(2):
            part = flipped[:, half * QB : (half + 1) * QB]
            spread = jnp.concatenate([part, jnp.zeros((KB, LINE - QB), F32)], axis=1)
            skewed = pltpu.roll(spread, 0, 1, stride=1, stride_axis=0)
            dline[2 * p + half] = jnp.sum(skewed, axis=0, keepdims=True)

    def settle(p):
        slot = lax.rem(p, 2)

        @pl.when(has_ahead)
        def _():
            grad_halo(p).wait_recv()
            kacc[slot, rows:, :] += halo_r[p, 0].astype(F32)
            vacc[slot, rows:, :] += halo_r[p, 1].astype(F32)

        for j, total in ((1, kacc), (2, vacc)):
            low = total[slot, HALO:, :].astype(BF)
            xw[:, aligned(p * 3 + j, LANES)] = low
            all_kv[p, own_rows, (j - 1) * LANES : j * LANES] = low

    def block_of(b):
        return slice(b * feat, (b + 1) * feat)

    def to_right(p, m, b):
        view = rights[m].at[p, b]
        return remote(view, view, rs_sem.at[m, p, b], rv_sem.at[m, p, b], at(z + 1, y, core))

    def to_left(p, m, b):
        view = lefts[m].at[p, b]
        return remote(view, view, ls_sem.at[m, p, b], lv_sem.at[m, p, b], at(z - 1, y, core))

    def hop(p, m, h):
        @pl.when(z == h)
        def _():
            for b in range(deep - 1, h, -1):
                total = zacc[p, block_of(b), lanes[m]]
                if h:
                    to_right(p, m, b).wait_recv()
                    total = total + rights[m][p, b].astype(F32)
                rights[m][p, b] = total.astype(BF)
                to_right(p, m, b).start()

        @pl.when(z == deep - 1 - h)
        def _():
            for b in range(0, deep - 1 - h):
                total = zacc[p, block_of(b), lanes[m]]
                if h:
                    to_left(p, m, b).wait_recv()
                    total = total + lefts[m][p, b].astype(F32)
                lefts[m][p, b] = total.astype(BF)
                to_left(p, m, b).start()

    def forward(p, m):
        for k in range(1, wide):
            to_wide(p, m, k).wait_recv()
            to_mate(p, m, k).start()

    def product(p, m):
        if m == 0:
            @pl.when(p == 0)
            def _():
                others = slice(0, (deep - zparts) * feat)
                some = xg.at[others, : (group - 1) * (rows - CHUNK)]
                pltpu.make_async_copy(some, some, gr_sem.at[1]).wait()
                some = xg.at[others, : rows - CHUNK]
                pltpu.make_async_copy(some, some, gl_sem.at[1]).wait()
                some = xg.at[others, : group * CHUNK]
                pltpu.make_async_copy(some, some, gr_sem.at[2]).wait()

        for k in range(wide):
            to_mate(p, m, k).wait_recv()
        zacc[p, : deep * feat, lanes[m]] = dot32(xg[...], alls[m][p], ((1,), (0,)))
        hop(p, m, 0)

    def finish(p, m):
        me = aligned(z, feat)

        @pl.when(z > 0)
        def _():
            to_right(p, m, z).wait_recv()
            zacc[p, me, lanes[m]] += rights[m][p, z].astype(F32)

        @pl.when(z < deep - 1)
        def _():
            to_left(p, m, z).wait_recv()
            zacc[p, me, lanes[m]] += lefts[m][p, z].astype(F32)

        total = zacc[p, me, lanes[m]]
        for j, ref in enumerate((dwk_ref, dwv_ref) if m else (dwq_ref,)):
            ref[:, aligned(p, LANES)] = total[:, j * LANES : (j + 1) * LANES]

    def near_copy(j, i):
        view = near.at[mine]
        return remote(
            view, view, bs_sem.at[0], br_sem.at[0], at(z, mod(y + j, wide), mod(core + i, 2))
        )

    def far_copy(k):
        view = far.at[z]
        return remote(view, view, bs_sem.at[1], br_sem.at[1], at(mod(z + k, deep), y, core))

    mates = [(j, i) for j in range(wide) for i in range(2) if i + j]

    def bias_near():
        near[mine] = jnp.concatenate([dline[n] for n in range(2 * pairs)], axis=0)
        for j, i in mates:
            near_copy(j, i).start()

    def bias_far():
        some = near.at[: group - 1]
        pltpu.make_async_copy(some, some, br_sem.at[0]).wait()
        total = near[0]
        for n in range(1, group):
            total = total + near[n]
        far[z] = total
        for k in range(1, deep):
            far_copy(k).start()

    tiles = dloc // TILE
    away = (tps - 1) * tiles

    def px_copy(j):
        return remote(
            pxs.at[j], pxr.at[j], ps_sem, pr_sem, (sp, mod(tp + 1 + lax.div(j, tiles), tps))
        )

    def input_tile(j):
        place = mod(tp + 1 + lax.div(j, tiles), tps) * tiles + lax.rem(j, tiles)
        low = dot32(
            xw[:, : pairs * TRIO], wcat[aligned(place, TILE), :], ((1,), (1,))
        ).astype(BF)

        @pl.when(j < away)
        def _():
            pxs[j] = low
            px_copy(j).start()

        @pl.when(j >= away)
        def _():
            gi_ref[:, aligned(j - away, TILE)] = low

    hops = deep - 2
    ready = pairs // 2
    last = 1 + 2 * (hops + 1)
    rounds = 3 * pairs - ready + last
    per = 2

    def staged(i, lag, stage):
        p = i - lag

        @pl.when((p >= 0) & (p < pairs))
        def _():
            stage(p)

    def pieced(i, lag, stage):
        n = i - lag
        odd = lax.rem(n + 2 * last, 2) == 1
        before = jnp.where(odd & (n > 0), lax.div(n - 1, 2), -1)
        piece = jnp.where(n < pairs, before, n - pairs + ready)
        for m in range(2):
            @pl.when((piece >= 0) & (piece < 2 * pairs) & (lax.rem(piece + 2, 2) == m))
            def _():
                stage(lax.div(piece, 2), m)

    @pl.loop(0, rounds)
    def _(i):
        staged(i, 0, attend)

        @pl.when(i == pairs - 1)
        def _():
            bias_near()

        staged(i, 1, settle)
        for m in range(2):
            @pl.when((i < pairs) & (lax.rem(i, 3) == m))
            def _():
                spread_out(lax.div(i, 3), m)

        @pl.when(i == pairs)
        def _():
            for p in range(pairs):
                for m in range(2):
                    if 3 * p + m >= pairs:
                        spread_out(p, m)

        pieced(i, 1, product)
        for h in range(1, hops + 1):
            pieced(i, 1 + 2 * h, functools.partial(hop, h=h))
        pieced(i, last, finish)
        pieced(i, 0, forward)

        @pl.when(i == pairs + 3)
        def _():
            bias_far()

        @pl.when(i >= pairs)
        def _():
            @pl.loop(0, per)
            def _(n):
                j = (i - pairs) * per + n

                @pl.when(j < tps * tiles)
                def _():
                    input_tile(j)

    some = far.at[: deep - 1]
    pltpu.make_async_copy(some, some, br_sem.at[1]).wait()
    summed = far[0]
    for n in range(1, deep):
        summed = summed + far[n]
    spot = lax.broadcasted_iota(jnp.int32, (rel_ref.shape[1], LINE), 1)
    back = bias_index(spot - (KB - 1))
    entry = lax.broadcasted_iota(jnp.int32, (rel_ref.shape[1], LINE), 0)
    gb_ref[...] = exact(summed, jnp.where(back == entry, 1.0, 0.0), ((1,), (1,)))

    pltpu.make_async_copy(pxr, pxr, pr_sem).wait()
    for n in range(tiles):
        cols = slice(n * TILE, (n + 1) * TILE)
        total = gi_ref[:, cols].astype(F32)
        for k in range(1, tps):
            total = total + pxr[(k - 1) * tiles + n].astype(F32)
        gi_ref[:, cols] = total.astype(BF)

    pltpu.make_async_copy(pxs, pxs, ps_sem).wait()
    for r in order:
        for k in range(1, tps):
            x_copy(k, r).wait_send()
    some = xg.at[: zparts * feat, : (group - 1) * rows]
    pltpu.make_async_copy(some, some, gs_sem.at[0]).wait()
    some = xg.at[: (deep - zparts) * feat, : (group - 1) * (rows - CHUNK)]
    pltpu.make_async_copy(some, some, gs_sem.at[1]).wait()
    some = xg.at[: (deep - zparts) * feat, : group * CHUNK]
    pltpu.make_async_copy(some, some, gs_sem.at[2]).wait()

    @pl.when(has_ahead)
    def _():
        halo_copy(k_ext, 0).wait_send()
        halo_copy(v_ext, 1).wait_send()

    for j, i in mates:
        near_copy(j, i).wait_send()
    for k in range(1, deep):
        far_copy(k).wait_send()

    @pl.loop(0, pairs)
    def _(p):
        @pl.when(has_behind)
        def _():
            grad_halo(p).wait_send()

        for m in range(2):
            for k in range(1, wide):
                to_wide(p, m, k).wait_send()
            for k in range(wide):
                to_mate(p, m, k).wait_send()
            for b in range(deep):
                @pl.when(z < b)
                def _():
                    to_right(p, m, b).wait_send()

                @pl.when(z > b)
                def _():
                    to_left(p, m, b).wait_send()


def local(sizes, inputs, w_query, w_key, w_value, rel_bias, d_out):
    seq, tps = sizes
    deep, wide = grid_of(seq // 2)
    rows, dloc = inputs.shape
    full, width = w_query.shape
    pairs = width // LANES
    ext = HALO + rows
    feat = full // seq
    group = 2 * wide
    tiles = dloc // TILE
    chunks = rows // CHUNK
    heads = rel_bias.shape[1]
    sds = jax.ShapeDtypeStruct
    vm = pltpu.VMEM
    dma = pltpu.SemaphoreType.DMA
    hbm = pl.BlockSpec(memory_space=pl.ANY)
    on_chip = pl.BlockSpec(memory_space=pltpu.VMEM)
    out = pl.pallas_call(
        functools.partial(step_body, sizes),
        in_specs=[hbm, hbm, hbm, hbm, on_chip, hbm],
        out_specs=[on_chip] * 5,
        out_shape=[
            sds((rows, dloc), BF),
            sds((feat, width), F32), sds((feat, width), F32), sds((feat, width), F32),
            sds((heads, rel_bias.shape[0]), F32),
        ],
        scratch_shapes=[
            vm((rows, full), BF),
            vm((full, pairs * TRIO), BF),
            vm((full, rows), BF),
            vm((deep * feat, group * rows), BF),
            vm((pairs, max(deep * feat, rows), TRIO), F32),
            vm((pairs, rows, LANES), BF),
            vm((pairs, ext, LANES), BF),
            vm((pairs, ext, LANES), BF),
            vm((pairs, rows, LANES), BF),
            vm((2 * pairs, 1, LINE), F32),
            vm((2 * pairs, 1, LINE), F32),
            vm((KB, 2 * QB), F32),
            vm((KB, 2 * QB), F32),
            vm((2, ext, LANES), F32),
            vm((2, ext, LANES), F32),
            vm((pairs, 2, HALO, LANES), BF),
            vm((pairs, 2, HALO, LANES), BF),
            vm((pairs, group * rows, LANES), BF),
            vm((pairs, group * rows, 2 * LANES), BF),
            vm((pairs, deep, feat, LANES), BF),
            vm((pairs, deep, feat, 2 * LANES), BF),
            vm((pairs, deep, feat, LANES), BF),
            vm((pairs, deep, feat, 2 * LANES), BF),
            vm(((tps - 1) * tiles, rows, TILE), BF),
            vm(((tps - 1) * tiles, rows, TILE), BF),
            vm((group, 2 * pairs, LINE), F32),
            vm((deep, 2 * pairs, LINE), F32),
            dma(()), dma(()), dma(()),
            dma((tps - 1, chunks)), dma((tps - 1, chunks)),
            dma((3,)), dma((3,)), dma((2,)),
            dma((2,)), dma((2,)),
            dma((pairs,)), dma((pairs,)),
            dma((2, pairs, wide - 1)), dma((2, pairs, wide - 1)),
            dma((2, pairs, wide)), dma((2, pairs, wide)),
            dma((2, pairs, deep)), dma((2, pairs, deep)),
            dma((2, pairs, deep)), dma((2, pairs, deep)),
            dma((2,)), dma((2,)),
            dma(()), dma(()),
        ],
        compiler_params=pltpu.CompilerParams(
            collective_id=0, has_side_effects=True, vmem_limit_bytes=67043328
        ),
        name="whole_step",
    )(inputs, w_query, w_key, w_value, rel_bias.T, d_out)
    return out[0], out[1], out[2], out[3], out[4].T


def solution(mesh):
    placed = (
        P("sp", "tp"),
        P(None, "tp"),
        P(None, "tp"),
        P(None, "tp"),
        P(None, "tp"),
        P("sp", "tp"),
    )
    sizes = (mesh.shape["sp"], mesh.shape["tp"])
    return jax.shard_map(
        functools.partial(local, sizes),
        mesh=mesh,
        in_specs=placed,
        out_specs=(P("sp", "tp"), P("sp", "tp"), P("sp", "tp"), P("sp", "tp"), P(None, "tp")),
        check_vma=False,
    )
```

```python
import functools

import jax
import jax.numpy as jnp
from jax import lax
from jax.experimental import pallas as pl
from jax.experimental.pallas import tpu as pltpu
from jax.sharding import PartitionSpec as P

HEAD = 64
SEG = 64
LEFT = 4
REL_MAX = 256
LANES = 128
QB = 2 * SEG
HALO = LEFT * SEG
KB = HALO + QB
LINE = 512
UNSEEN = -1e30
CHUNK = 128
TILE = 256
TRIO = 3 * LANES
MESH = pl.DeviceIdType.MESH
BF = jnp.bfloat16
F32 = jnp.float32


def dot32(a, b, dims):
    return lax.dot_general(a, b, (dims, ((), ())), preferred_element_type=F32)


def exact(a, b, dims):
    return lax.dot_general(
        a, b, (dims, ((), ())), precision=lax.Precision.HIGHEST, preferred_element_type=F32
    )


def grid_of(chips):
    depth = 1
    while depth * depth < chips:
        depth *= 2
    return depth, chips // depth


def aligned(index, size):
    return pl.ds(pl.multiple_of(index * size, size), size)


def bias_index(apart):
    return jnp.clip(HALO + apart, 1 - SEG, REL_MAX) + SEG - 1


def step_body(
    sizes,
    x_ref, wq_ref, wk_ref, wv_ref, rel_ref, d_ref,
    gi_out, dw_out, gb_out,
    xw, wcat, xt, xg, zacc, q_s, k_ext, v_ext, d_s, lines, dline, bias, bias_sum, kacc, vacc,
    halo_s, halo_r, all_q, all_kv, right_q, right_kv, left_q, left_kv, pxs, pxr, near, far,
    xl, gi_ref, dw_ref, gb_ref, o_sem,
    w_sem, d_sem, x_sem, xs_sem, xr_sem, gs_sem, gr_sem, gl_sem, ks_sem, kr_sem, hs_sem, hr_sem,
    ys_sem, yr_sem, cs_sem, cr_sem, rs_sem, rv_sem, ls_sem, lv_sem, bs_sem, br_sem, ps_sem, pr_sem,
):
    alls, rights, lefts = (all_q, all_kv), (right_q, right_kv), (left_q, left_kv)
    lanes = (slice(0, LANES), slice(LANES, TRIO))
    seq, tps = sizes
    deep, wide = grid_of(seq // 2)
    rows, dloc = x_ref.shape
    pairs = wq_ref.shape[1] // LANES
    ext = HALO + rows
    blocks = rows // QB
    feat = dloc * tps // seq
    group = 2 * wide
    sp = lax.axis_index("sp")
    tp = lax.axis_index("tp")
    core = lax.rem(sp, 2)
    chip = lax.div(sp, 2)
    y = lax.rem(chip, wide)
    z = lax.div(chip, wide)
    mine = y * 2 + core

    def at(zi, yi, ci):
        return ((zi * wide + yi) * 2 + ci, tp)

    def mod(a, n):
        return lax.rem(a + n, n)

    mate = at(z, y, 1 - core)
    ahead, behind = (sp + 1, tp), (sp - 1, tp)
    has_ahead, has_behind = sp + 1 < seq, sp > 0

    greeted = [(sp, mod(tp + k, tps)) for k in range(1, tps)]
    greeted += [(mod(sp + 1, seq), tp), (mod(sp - 1, seq), tp)]
    greeted += [at(z, mod(y + j, wide), mod(core + i, 2)) for j in range(wide) for i in range(2) if i + j]
    greeted += [at(mod(z + k, deep), y, core) for k in range(1, deep)]
    barrier = pltpu.get_barrier_semaphore()
    for other in greeted:
        pl.semaphore_signal(barrier, inc=1, device_id=other, device_id_type=MESH)

    own_x = pltpu.make_async_copy(x_ref, xw.at[:, aligned(tp, dloc)], x_sem)
    own_x.start()
    for p in range(pairs):
        for j, w_ref in enumerate((wq_ref, wk_ref, wv_ref)):
            pltpu.make_async_copy(
                w_ref.at[:, p * LANES : (p + 1) * LANES],
                wcat.at[:, p * TRIO + j * LANES : p * TRIO + (j + 1) * LANES], w_sem,
            ).start()
    for p in range(pairs):
        pltpu.make_async_copy(
            d_ref.at[:, p * LANES : (p + 1) * LANES], d_s.at[p], d_sem
        ).start()
    pl.semaphore_wait(barrier, len(greeted))

    def remote(src, dst, send, recv, device):
        return pltpu.make_async_remote_copy(
            src_ref=src, dst_ref=dst, send_sem=send, recv_sem=recv,
            device_id=device, device_id_type=MESH,
        )

    chunks = rows // CHUNK
    first = (rows - HALO) // CHUNK
    order = list(range(first, chunks)) + list(range(first))

    def x_copy(k, r):
        part = slice(r * CHUNK, (r + 1) * CHUNK)
        landing = xl.at[k - 1] if r == order[-1] else xw.at[part, aligned(tp, dloc)]
        return remote(
            x_ref.at[part, :], landing,
            xs_sem.at[k - 1, r], xr_sem.at[k - 1, r], (sp, mod(tp + k, tps)),
        )

    for r in order:
        for k in range(1, tps):
            x_copy(k, r).start()
    own_x.wait()

    def turn(t, r, source=None):
        part = slice(r * CHUNK, (r + 1) * CHUNK)

        @pl.loop(0, dloc // TILE)
        def _(f):
            cols = aligned(t * (dloc // TILE) + f, TILE)
            if source is None:
                xt[cols, part] = xw[part, cols].T
            else:
                xt[cols, part] = xl[source, :, aligned(f, TILE)].T

    zparts = deep // tps

    def share(t, low, high, own, afar=True):
        for j in range(wide):
            for i in range(2):
                for q in range(zparts):
                    zb = t * zparts + q
                    y2, c2 = mod(y + j, wide), mod(core + i, 2)
                    src = xt.at[aligned((zb * wide + y2) * 2 + c2, feat), low:high]
                    cols = pl.ds(pl.multiple_of(mine * rows + low, CHUNK), high - low)
                    dst = xg.at[aligned(zb, feat), cols]
                    if i + j and not afar:
                        continue
                    if i + j:
                        remote(src, dst, gs_sem.at[own], gr_sem.at[own], at(z, y2, c2)).start()
                    else:
                        pltpu.make_async_copy(src, dst, gl_sem.at[own]).start()

    for r in range(chunks):
        turn(tp, r)
        share(tp, r * CHUNK, (r + 1) * CHUNK, 0)

    pltpu.make_async_copy(wcat, wcat, w_sem).wait()

    @pl.loop(0, pairs)
    def _(p):
        zacc[p, :rows, :] = dot32(
            xw[:, aligned(tp, dloc)], wcat[aligned(tp, dloc), aligned(p, TRIO)], ((1,), (0,))
        )

    @pl.when(sp == 0)
    def _():
        k_ext[:, :HALO, :] = jnp.zeros((pairs, HALO, LANES), BF)
        v_ext[:, :HALO, :] = jnp.zeros((pairs, HALO, LANES), BF)

    spot = lax.broadcasted_iota(jnp.int32, (rel_ref.shape[1], LINE), 1)
    entry = lax.broadcasted_iota(jnp.int32, (rel_ref.shape[1], LINE), 0)
    apart = jnp.where(spot < QB, spot, spot - LINE)
    picked = exact(rel_ref[...], jnp.where(bias_index(apart) == entry, 1.0, 0.0), ((1,), (0,)))
    for n in range(2 * pairs):
        lines[n] = picked[n : n + 1, :]

    def halo_copy(ref, n):
        return remote(
            ref.at[:, rows : rows + HALO, :], ref.at[:, :HALO, :],
            ks_sem.at[n], kr_sem.at[n], ahead,
        )

    def cross_copy(k, g):
        cols = pl.ds(pl.multiple_of(mod(mine + g, group) * rows, rows), rows - HALO)
        view = xg.at[aligned(tp, zparts * feat), cols]
        return remote(view, view, gs_sem.at[2], gr_sem.at[2], (sp, mod(tp + k, tps)))

    def project(p, r):
        part = slice(r * CHUNK, (r + 1) * CHUNK)
        total = zacc[p, part, :]
        for k in range(1, tps):
            t = mod(tp - k, tps)
            whole = xl[k - 1] if r == order[-1] else xw[part, aligned(t, dloc)]
            total = total + dot32(
                whole, wcat[aligned(t, dloc), aligned(p, TRIO)], ((1,), (0,))
            )
        low = total.astype(BF)
        q_s[p, part, :] = low[:, :LANES]
        k_ext[p, HALO + r * CHUNK : HALO + (r + 1) * CHUNK, :] = low[:, LANES : 2 * LANES]
        v_ext[p, HALO + r * CHUNK : HALO + (r + 1) * CHUNK, :] = low[:, 2 * LANES :]

    early = chunks - first - 1
    for n, r in enumerate(order):
        for k in range(1, tps):
            x_copy(k, r).wait_recv()

        if n == chunks - 1:
            some = xg.at[: zparts * feat, : (group - 1) * rows]
            pltpu.make_async_copy(some, some, gr_sem.at[0]).wait()
            some = xg.at[: zparts * feat, :rows]
            pltpu.make_async_copy(some, some, gl_sem.at[0]).wait()
            for k in range(1, tps):
                for g in range(1, group):
                    cross_copy(k, g).start()

        if n < chunks - 1:
            @pl.loop(0, pairs)
            def _(p):
                project(p, r)

        if n == early:
            @pl.when(has_ahead)
            def _():
                halo_copy(k_ext, 0).start()
                halo_copy(v_ext, 1).start()

        for k in range(1, tps):
            t = mod(tp - k, tps)
            if n < chunks - 1:
                turn(t, r)
            if n == min(early + 1, chunks - 1):
                for done in order[: early + 1]:
                    share(t, done * CHUNK, (done + 1) * CHUNK, 1)
            if early < n < chunks - 1:
                share(t, r * CHUNK, (r + 1) * CHUNK, 1, afar=False)

    pltpu.make_async_copy(d_s, d_s, d_sem).wait()

    @pl.when(has_behind)
    def _():
        halo_copy(k_ext, 0).wait_recv()
        halo_copy(v_ext, 1).wait_recv()

    key_row = lax.broadcasted_iota(jnp.int32, (KB, QB), 0)
    query_row = lax.broadcasted_iota(jnp.int32, (KB, QB), 1)
    lane = lax.broadcasted_iota(jnp.int32, (QB, LANES), 1)
    scale = HEAD ** (-0.5)
    zero = jnp.zeros((QB, LANES), BF)
    own_rows = aligned(mine, rows)

    def stacked(part):
        return jnp.concatenate(
            [jnp.where(lane < HEAD, part, zero), jnp.where(lane < HEAD, zero, part)], axis=0
        )

    def grad_halo(p):
        return remote(halo_s.at[p], halo_r.at[p], hs_sem.at[p], hr_sem.at[p], behind)

    def to_wide(p, m, k):
        view = alls[m].at[p, own_rows, :]
        return remote(
            view, view, ys_sem.at[m, p, k - 1], yr_sem.at[m, p, k - 1],
            at(z, mod(y + k, wide), core),
        )

    def to_mate(p, m, k):
        owner = aligned(mod(y - k, wide) * 2 + core, rows)
        view = alls[m].at[p, owner, :]
        return remote(view, view, cs_sem.at[m, p, k], cr_sem.at[m, p, k], mate)

    def spread_out(p, m):
        for k in range(1, wide):
            to_wide(p, m, k).start()
        to_mate(p, m, 0).start()

    def attend(p):
        project(p, order[-1])
        slot = lax.rem(p, 2)
        offset = key_row - jnp.where(query_row < SEG, 0, SEG)
        seen = (offset >= 0) & (offset < HALO + SEG)
        for half in range(2):
            line = jnp.broadcast_to(lines[2 * p + half], (KB, LINE))
            skewed = pltpu.roll(line, 0, 1, stride=1, stride_axis=0)[:, :QB]
            bias[:, half * QB : (half + 1) * QB] = jnp.where(seen, skewed, UNSEEN)
        kacc[slot] = jnp.zeros((ext, LANES), F32)
        vacc[slot] = jnp.zeros((ext, LANES), F32)
        bias_sum[...] = jnp.zeros_like(bias_sum)
        for block in range(blocks):
            keys = slice(block * QB, block * QB + KB)
            part = slice(block * QB, (block + 1) * QB)
            q2 = stacked(q_s[p, part, :] * BF(scale))
            d2 = stacked(d_s[p, part, :])
            k = k_ext[p, keys, :]
            v = v_ext[p, keys, :]
            score = dot32(k, q2, ((1,), (1,))) + bias[...]
            if block * QB < HALO:
                row = lax.broadcasted_iota(jnp.int32, (KB, 1), 0) + block * QB
                score = score + jnp.where((row < HALO) & (sp == 0), UNSEEN, 0.0)
            top = jnp.max(score, axis=0, keepdims=True)
            power = jnp.exp(score - top)
            prob = power * (1.0 / jnp.sum(power, axis=0, keepdims=True))
            prob_low = prob.astype(BF)
            grad_prob = dot32(v, d2, ((1,), (1,)))
            delta = jnp.sum(prob_low.astype(F32) * grad_prob, axis=0, keepdims=True)
            dscore = prob * (grad_prob - delta)
            bias_sum[...] += dscore
            dscore_low = dscore.astype(BF)
            vacc[slot, keys, :] += dot32(prob_low, d2, ((1,), (0,)))
            kacc[slot, keys, :] += dot32(dscore_low, q2, ((1,), (0,)))
            dq_t = dot32(k, dscore_low, ((0,), (0,)))
            dq_t = jnp.concatenate([dq_t[:HEAD, :QB], dq_t[HEAD:, QB:]], axis=0)
            dq = (dq_t.T * scale).astype(BF)
            xw[part, aligned(p * 3, LANES)] = dq
            all_q[p, pl.ds(pl.multiple_of(mine * rows + block * QB, QB), QB), :] = dq
            if block == HALO // QB - 1:
                halo_s[p, 0] = kacc[slot, :HALO, :].astype(BF)
                halo_s[p, 1] = vacc[slot, :HALO, :].astype(BF)

                @pl.when(has_behind)
                def _():
                    grad_halo(p).start()

        flip_row = lax.broadcasted_iota(jnp.int32, (KB, KB), 0)
        flip_col = lax.broadcasted_iota(jnp.int32, (KB, KB), 1)
        flip = jnp.where(flip_row + flip_col == KB - 1, 1.0, 0.0)
        flipped = exact(flip, bias_sum[...], ((1,), (0,)))
        for half in range(2):
            part = flipped[:, half * QB : (half + 1) * QB]
            spread = jnp.concatenate([part, jnp.zeros((KB, LINE - QB), F32)], axis=1)
            skewed = pltpu.roll(spread, 0, 1, stride=1, stride_axis=0)
            dline[2 * p + half] = jnp.sum(skewed, axis=0, keepdims=True)

    def settle(p):
        slot = lax.rem(p, 2)

        @pl.when(has_ahead)
        def _():
            grad_halo(p).wait_recv()
            kacc[slot, rows:, :] += halo_r[p, 0].astype(F32)
            vacc[slot, rows:, :] += halo_r[p, 1].astype(F32)

        for j, total in ((1, kacc), (2, vacc)):
            low = total[slot, HALO:, :].astype(BF)
            xw[:, aligned(p * 3 + j, LANES)] = low
            all_kv[p, own_rows, (j - 1) * LANES : j * LANES] = low

    def block_of(b):
        return slice(b * feat, (b + 1) * feat)

    def to_right(p, m, b):
        view = rights[m].at[p, b]
        return remote(view, view, rs_sem.at[m, p, b], rv_sem.at[m, p, b], at(z + 1, y, core))

    def to_left(p, m, b):
        view = lefts[m].at[p, b]
        return remote(view, view, ls_sem.at[m, p, b], lv_sem.at[m, p, b], at(z - 1, y, core))

    def hop(p, m, h):
        @pl.when(z == h)
        def _():
            for b in range(deep - 1, h, -1):
                total = zacc[p, block_of(b), lanes[m]]
                if h:
                    to_right(p, m, b).wait_recv()
                    total = total + rights[m][p, b].astype(F32)
                rights[m][p, b] = total.astype(BF)
                to_right(p, m, b).start()

        @pl.when(z == deep - 1 - h)
        def _():
            for b in range(0, deep - 1 - h):
                total = zacc[p, block_of(b), lanes[m]]
                if h:
                    to_left(p, m, b).wait_recv()
                    total = total + lefts[m][p, b].astype(F32)
                lefts[m][p, b] = total.astype(BF)
                to_left(p, m, b).start()

    def forward(p, m):
        for k in range(1, wide):
            to_wide(p, m, k).wait_recv()
            to_mate(p, m, k).start()

    def product(p, m):
        if m == 0:
            @pl.when(p == 0)
            def _():
                others = slice(0, (deep - zparts) * feat)
                some = xg.at[others, : (group - 1) * HALO]
                pltpu.make_async_copy(some, some, gr_sem.at[1]).wait()
                some = xg.at[others, :rows]
                pltpu.make_async_copy(some, some, gl_sem.at[1]).wait()
                some = xg.at[others, : (group - 1) * (rows - HALO)]
                pltpu.make_async_copy(some, some, gr_sem.at[2]).wait()

        for k in range(wide):
            to_mate(p, m, k).wait_recv()
        zacc[p, : deep * feat, lanes[m]] = dot32(xg[...], alls[m][p], ((1,), (0,)))
        hop(p, m, 0)

    def grad_out(p, j):
        cols = aligned(p, LANES)
        return pltpu.make_async_copy(dw_ref.at[j, :, cols], dw_out.at[j, :, cols], o_sem.at[0])

    def finish(p, m):
        me = aligned(z, feat)

        @pl.when(z > 0)
        def _():
            to_right(p, m, z).wait_recv()
            zacc[p, me, lanes[m]] += rights[m][p, z].astype(F32)

        @pl.when(z < deep - 1)
        def _():
            to_left(p, m, z).wait_recv()
            zacc[p, me, lanes[m]] += lefts[m][p, z].astype(F32)

        total = zacc[p, me, lanes[m]]
        for j in range(1 + m):
            dw_ref[m + j, :, aligned(p, LANES)] = total[:, j * LANES : (j + 1) * LANES]
            grad_out(p, m + j).start()

    def near_copy(j, i):
        view = near.at[mine]
        return remote(
            view, view, bs_sem.at[0], br_sem.at[0], at(z, mod(y + j, wide), mod(core + i, 2))
        )

    def far_copy(k):
        view = far.at[z]
        return remote(view, view, bs_sem.at[1], br_sem.at[1], at(mod(z + k, deep), y, core))

    mates = [(j, i) for j in range(wide) for i in range(2) if i + j]

    def bias_near():
        near[mine] = jnp.concatenate([dline[n] for n in range(2 * pairs)], axis=0)
        for j, i in mates:
            near_copy(j, i).start()

    def bias_far():
        some = near.at[: group - 1]
        pltpu.make_async_copy(some, some, br_sem.at[0]).wait()
        total = near[0]
        for n in range(1, group):
            total = total + near[n]
        far[z] = total
        for k in range(1, deep):
            far_copy(k).start()

    tiles = dloc // TILE
    away = (tps - 1) * tiles

    def px_copy(j):
        return remote(
            pxs.at[j], pxr.at[j], ps_sem, pr_sem, (sp, mod(tp + 1 + lax.div(j, tiles), tps))
        )

    def input_tile(j):
        place = mod(tp + 1 + lax.div(j, tiles), tps) * tiles + lax.rem(j, tiles)
        low = dot32(
            xw[:, : pairs * TRIO], wcat[aligned(place, TILE), :], ((1,), (1,))
        ).astype(BF)

        @pl.when(j < away)
        def _():
            pxs[j] = low
            px_copy(j).start()

        @pl.when(j >= away)
        def _():
            gi_ref[:, aligned(j - away, TILE)] = low

    hops = deep - 2
    early_pieces = pairs - 1
    last = 3 + 2 * (hops + 1)
    rounds = 2 * pairs + last
    per = 2

    def staged(i, lag, stage):
        p = i - lag

        @pl.when((p >= 0) & (p < pairs))
        def _():
            stage(p)

    def pieced(i, lag, stage):
        piece = i - lag
        valid = (piece >= 0) & (piece < 2 * pairs)
        mixed = piece < early_pieces
        kv_left = pairs - early_pieces // 2
        parity = lax.rem(piece + 2 * last, 2)
        is_kv = jnp.where(mixed, parity, jnp.where(piece < early_pieces + kv_left, 1, 0))
        late_pair = jnp.where(is_kv == 1, piece - early_pieces + early_pieces // 2, piece - pairs)
        pair = jnp.where(mixed, lax.div(piece, 2), late_pair)
        for m in range(2):
            @pl.when(valid & (is_kv == m))
            def _():
                stage(pair, m)

    @pl.loop(0, rounds)
    def _(i):
        staged(i, 0, attend)

        @pl.when(i == pairs - 1)
        def _():
            bias_near()

        staged(i, 1, settle)
        for m in range(2):
            @pl.when((i < early_pieces) & (lax.rem(i, 2) == m))
            def _():
                spread_out(lax.div(i, 2), m)

        @pl.when(i == 0)
        def _():
            for k in range(1, tps):
                r = order[-1]
                turn(mod(tp - k, tps), r, k - 1)
                share(mod(tp - k, tps), r * CHUNK, (r + 1) * CHUNK, 1, afar=False)

        @pl.when(i == pairs)
        def _():
            for m in (1, 0):
                for p in range(pairs):
                    if 2 * p + m >= early_pieces:
                        spread_out(p, m)

        pieced(i, 3, product)
        for h in range(1, hops + 1):
            pieced(i, 3 + 2 * h, functools.partial(hop, h=h))
        pieced(i, last, finish)
        pieced(i, 2, forward)

        @pl.when(i == pairs + 3)
        def _():
            bias_far()

        @pl.when(i >= pairs)
        def _():
            @pl.loop(0, per)
            def _(n):
                j = (i - pairs) * per + n

                @pl.when(j < tps * tiles)
                def _():
                    input_tile(j)

    some = far.at[: deep - 1]
    pltpu.make_async_copy(some, some, br_sem.at[1]).wait()
    summed = far[0]
    for n in range(1, deep):
        summed = summed + far[n]
    spot = lax.broadcasted_iota(jnp.int32, (rel_ref.shape[1], LINE), 1)
    back = bias_index(spot - (KB - 1))
    entry = lax.broadcasted_iota(jnp.int32, (rel_ref.shape[1], LINE), 0)
    gb_ref[...] = exact(summed, jnp.where(back == entry, 1.0, 0.0), ((1,), (1,)))

    pltpu.make_async_copy(gb_ref, gb_out, o_sem.at[2]).start()
    pltpu.make_async_copy(pxr, pxr, pr_sem).wait()
    for n in range(tiles):
        cols = slice(n * TILE, (n + 1) * TILE)
        total = gi_ref[:, cols].astype(F32)
        for k in range(1, tps):
            total = total + pxr[(k - 1) * tiles + n].astype(F32)
        gi_ref[:, cols] = total.astype(BF)
        pltpu.make_async_copy(gi_ref.at[:, cols], gi_out.at[:, cols], o_sem.at[1]).start()

    pltpu.make_async_copy(pxs, pxs, ps_sem).wait()
    for r in order:
        for k in range(1, tps):
            x_copy(k, r).wait_send()
    some = xg.at[: zparts * feat, : (group - 1) * rows]
    pltpu.make_async_copy(some, some, gs_sem.at[0]).wait()
    some = xg.at[: (deep - zparts) * feat, : (group - 1) * HALO]
    pltpu.make_async_copy(some, some, gs_sem.at[1]).wait()
    some = xg.at[: (deep - zparts) * feat, : (group - 1) * (rows - HALO)]
    pltpu.make_async_copy(some, some, gs_sem.at[2]).wait()

    @pl.when(has_ahead)
    def _():
        halo_copy(k_ext, 0).wait_send()
        halo_copy(v_ext, 1).wait_send()

    for j, i in mates:
        near_copy(j, i).wait_send()
    for k in range(1, deep):
        far_copy(k).wait_send()

    @pl.loop(0, pairs)
    def _(p):
        @pl.when(has_behind)
        def _():
            grad_halo(p).wait_send()

        for m in range(2):
            for k in range(1, wide):
                to_wide(p, m, k).wait_send()
            for k in range(wide):
                to_mate(p, m, k).wait_send()
            for b in range(deep):
                @pl.when(z < b)
                def _():
                    to_right(p, m, b).wait_send()

                @pl.when(z > b)
                def _():
                    to_left(p, m, b).wait_send()

    pltpu.make_async_copy(dw_ref, dw_out, o_sem.at[0]).wait()
    pltpu.make_async_copy(gi_ref, gi_out, o_sem.at[1]).wait()
    pltpu.make_async_copy(gb_ref, gb_out, o_sem.at[2]).wait()


def hand_body(gi, dw, gb, gi_out, dwq_out, dwk_out, dwv_out, gb_out, gi_v, dw_v, gb_v, i_sem, o_sem):
    outs = (dwq_out, dwk_out, dwv_out)
    rows = gi.shape[0] // 2
    moves = [(gi.at[n * rows : (n + 1) * rows], gi_v.at[n * rows : (n + 1) * rows],
              gi_out.at[n * rows : (n + 1) * rows]) for n in range(2)]
    moves += [(dw.at[j], dw_v.at[j], outs[j]) for j in range(3)]
    moves.append((gb, gb_v, gb_out))
    for n, (src, mid, _) in enumerate(moves):
        pltpu.make_async_copy(src, mid, i_sem.at[n]).start()
    for n, (src, mid, dst) in enumerate(moves):
        pltpu.make_async_copy(src, mid, i_sem.at[n]).wait()
        pltpu.make_async_copy(mid, dst, o_sem.at[n]).start()
    for n, (_, mid, dst) in enumerate(moves):
        pltpu.make_async_copy(mid, dst, o_sem.at[n]).wait()


def local(sizes, inputs, w_query, w_key, w_value, rel_bias, d_out):
    seq, tps = sizes
    deep, wide = grid_of(seq // 2)
    rows, dloc = inputs.shape
    full, width = w_query.shape
    pairs = width // LANES
    ext = HALO + rows
    feat = full // seq
    group = 2 * wide
    tiles = dloc // TILE
    chunks = rows // CHUNK
    heads = rel_bias.shape[1]
    sds = jax.ShapeDtypeStruct
    vm = pltpu.VMEM
    dma = pltpu.SemaphoreType.DMA
    hbm = pl.BlockSpec(memory_space=pl.ANY)
    on_chip = pl.BlockSpec(memory_space=pltpu.VMEM)
    out = pl.pallas_call(
        functools.partial(step_body, sizes),
        in_specs=[hbm, hbm, hbm, hbm, on_chip, hbm],
        out_specs=[hbm] * 3,
        out_shape=[
            sds((rows, dloc), BF),
            sds((3, feat, width), F32),
            sds((heads, rel_bias.shape[0]), F32),
        ],
        scratch_shapes=[
            vm((rows, full), BF),
            vm((full, pairs * TRIO), BF),
            vm((full, rows), BF),
            vm((deep * feat, group * rows), BF),
            vm((pairs, max(deep * feat, rows), TRIO), F32),
            vm((pairs, rows, LANES), BF),
            vm((pairs, ext, LANES), BF),
            vm((pairs, ext, LANES), BF),
            vm((pairs, rows, LANES), BF),
            vm((2 * pairs, 1, LINE), F32),
            vm((2 * pairs, 1, LINE), F32),
            vm((KB, 2 * QB), F32),
            vm((KB, 2 * QB), F32),
            vm((2, ext, LANES), F32),
            vm((2, ext, LANES), F32),
            vm((pairs, 2, HALO, LANES), BF),
            vm((pairs, 2, HALO, LANES), BF),
            vm((pairs, group * rows, LANES), BF),
            vm((pairs, group * rows, 2 * LANES), BF),
            vm((pairs, deep, feat, LANES), BF),
            vm((pairs, deep, feat, 2 * LANES), BF),
            vm((pairs, deep, feat, LANES), BF),
            vm((pairs, deep, feat, 2 * LANES), BF),
            vm(((tps - 1) * tiles, rows, TILE), BF),
            vm(((tps - 1) * tiles, rows, TILE), BF),
            vm((group, 2 * pairs, LINE), F32),
            vm((deep, 2 * pairs, LINE), F32),
            vm((tps - 1, CHUNK, dloc), BF),
            vm((rows, dloc), BF),
            vm((3, feat, width), F32),
            vm((heads, rel_bias.shape[0]), F32),
            dma((3,)),
            dma(()), dma(()), dma(()),
            dma((tps - 1, chunks)), dma((tps - 1, chunks)),
            dma((3,)), dma((3,)), dma((2,)),
            dma((2,)), dma((2,)),
            dma((pairs,)), dma((pairs,)),
            dma((2, pairs, wide - 1)), dma((2, pairs, wide - 1)),
            dma((2, pairs, wide)), dma((2, pairs, wide)),
            dma((2, pairs, deep)), dma((2, pairs, deep)),
            dma((2, pairs, deep)), dma((2, pairs, deep)),
            dma((2,)), dma((2,)),
            dma(()), dma(()),
        ],
        compiler_params=pltpu.CompilerParams(
            collective_id=0, has_side_effects=True, vmem_limit_bytes=67043328
        ),
        name="whole_step",
    )(inputs, w_query, w_key, w_value, rel_bias.T, d_out)
    grad = sds((feat, width), F32)
    out = pl.pallas_call(
        hand_body,
        in_specs=[hbm] * 3,
        out_specs=[hbm] * 5,
        out_shape=[sds((rows, dloc), BF), grad, grad, grad, sds((heads, rel_bias.shape[0]), F32)],
        scratch_shapes=[
            vm((rows, dloc), BF), vm((3, feat, width), F32), vm((heads, rel_bias.shape[0]), F32),
            dma((6,)), dma((6,)),
        ],
        name="hand_out",
    )(*out)
    return out[0], out[1], out[2], out[3], out[4].T


def solution(mesh):
    placed = (
        P("sp", "tp"),
        P(None, "tp"),
        P(None, "tp"),
        P(None, "tp"),
        P(None, "tp"),
        P("sp", "tp"),
    )
    sizes = (mesh.shape["sp"], mesh.shape["tp"])
    return jax.shard_map(
        functools.partial(local, sizes),
        mesh=mesh,
        in_specs=placed,
        out_specs=(P("sp", "tp"), P("sp", "tp"), P("sp", "tp"), P("sp", "tp"), P(None, "tp")),
        check_vma=False,
    )
```

```python
import functools

import jax
import jax.numpy as jnp
from jax import lax
from jax.experimental import pallas as pl
from jax.experimental.pallas import tpu as pltpu
from jax.sharding import PartitionSpec as P

HEAD = 64
SEG = 64
LEFT = 4
REL_MAX = 256
LANES = 128
QB = 2 * SEG
HALO = LEFT * SEG
KB = HALO + QB
LINE = 512
UNSEEN = -1e30
CHUNK = 128
TILE = 256
TRIO = 3 * LANES
MESH = pl.DeviceIdType.MESH
BF = jnp.bfloat16
F32 = jnp.float32


def dot32(a, b, dims):
    return lax.dot_general(a, b, (dims, ((), ())), preferred_element_type=F32)


def exact(a, b, dims):
    return lax.dot_general(
        a, b, (dims, ((), ())), precision=lax.Precision.HIGHEST, preferred_element_type=F32
    )


def grid_of(chips):
    depth = 1
    while depth * depth < chips:
        depth *= 2
    return depth, chips // depth


def aligned(index, size):
    return pl.ds(pl.multiple_of(index * size, size), size)


def bias_index(apart):
    return jnp.clip(HALO + apart, 1 - SEG, REL_MAX) + SEG - 1


def step_body(
    sizes,
    x_ref, wq_ref, wk_ref, wv_ref, rel_ref, d_ref,
    gi_out, dw_out, gb_out,
    xw, wcat, xt, xg, zacc, q_s, k_ext, v_ext, d_s, lines, dline, bias, bias_sum, kacc, vacc,
    halo_s, halo_r, all_q, all_kv, right_q, right_kv, left_q, left_kv, pxs, pxr, near, far,
    xl, gi_ref, dw_ref, gb_ref, o_sem,
    w_sem, d_sem, x_sem, xs_sem, xr_sem, gs_sem, gr_sem, gl_sem, ks_sem, kr_sem, hs_sem, hr_sem,
    ys_sem, yr_sem, cs_sem, cr_sem, rs_sem, rv_sem, ls_sem, lv_sem, bs_sem, br_sem, ps_sem, pr_sem,
):
    alls, rights, lefts = (all_q, all_kv), (right_q, right_kv), (left_q, left_kv)
    lanes = (slice(0, LANES), slice(LANES, TRIO))
    seq, tps = sizes
    deep, wide = grid_of(seq // 2)
    rows, dloc = x_ref.shape
    pairs = wq_ref.shape[1] // LANES
    ext = HALO + rows
    blocks = rows // QB
    feat = dloc * tps // seq
    group = 2 * wide
    sp = lax.axis_index("sp")
    tp = lax.axis_index("tp")
    core = lax.rem(sp, 2)
    chip = lax.div(sp, 2)
    y = lax.rem(chip, wide)
    z = lax.div(chip, wide)
    mine = y * 2 + core

    def at(zi, yi, ci):
        return ((zi * wide + yi) * 2 + ci, tp)

    def mod(a, n):
        return lax.rem(a + n, n)

    mate = at(z, y, 1 - core)
    ahead, behind = (sp + 1, tp), (sp - 1, tp)
    has_ahead, has_behind = sp + 1 < seq, sp > 0

    greeted = [(sp, mod(tp + k, tps)) for k in range(1, tps)]
    greeted += [(mod(sp + 1, seq), tp), (mod(sp - 1, seq), tp)]
    greeted += [at(z, mod(y + j, wide), mod(core + i, 2)) for j in range(wide) for i in range(2) if i + j]
    greeted += [at(mod(z + k, deep), y, core) for k in range(1, deep)]
    barrier = pltpu.get_barrier_semaphore()
    for other in greeted:
        pl.semaphore_signal(barrier, inc=1, device_id=other, device_id_type=MESH)

    own_x = pltpu.make_async_copy(x_ref, xw.at[:, aligned(tp, dloc)], x_sem)
    own_x.start()
    for p in range(pairs):
        for j, w_ref in enumerate((wq_ref, wk_ref, wv_ref)):
            pltpu.make_async_copy(
                w_ref.at[:, p * LANES : (p + 1) * LANES],
                wcat.at[:, p * TRIO + j * LANES : p * TRIO + (j + 1) * LANES], w_sem,
            ).start()
    for p in range(pairs):
        pltpu.make_async_copy(
            d_ref.at[:, p * LANES : (p + 1) * LANES], d_s.at[p], d_sem
        ).start()
    pl.semaphore_wait(barrier, len(greeted))

    def remote(src, dst, send, recv, device):
        return pltpu.make_async_remote_copy(
            src_ref=src, dst_ref=dst, send_sem=send, recv_sem=recv,
            device_id=device, device_id_type=MESH,
        )

    chunks = rows // CHUNK
    first = (rows - HALO) // CHUNK
    order = list(range(first, chunks)) + list(range(first))

    def x_copy(k, r):
        part = slice(r * CHUNK, (r + 1) * CHUNK)
        landing = xl.at[k - 1] if r == order[-1] else xw.at[part, aligned(tp, dloc)]
        return remote(
            x_ref.at[part, :], landing,
            xs_sem.at[k - 1, r], xr_sem.at[k - 1, r], (sp, mod(tp + k, tps)),
        )

    for r in order:
        for k in range(1, tps):
            x_copy(k, r).start()
    own_x.wait()

    def turn(t, r, source=None):
        part = slice(r * CHUNK, (r + 1) * CHUNK)

        @pl.loop(0, dloc // TILE)
        def _(f):
            cols = aligned(t * (dloc // TILE) + f, TILE)
            if source is None:
                xt[cols, part] = xw[part, cols].T
            else:
                xt[cols, part] = xl[source, :, aligned(f, TILE)].T

    zparts = deep // tps

    def share(t, low, high, own, afar=True):
        for j in range(wide):
            for i in range(2):
                for q in range(zparts):
                    zb = t * zparts + q
                    y2, c2 = mod(y + j, wide), mod(core + i, 2)
                    src = xt.at[aligned((zb * wide + y2) * 2 + c2, feat), low:high]
                    cols = pl.ds(pl.multiple_of(mine * rows + low, CHUNK), high - low)
                    dst = xg.at[aligned(zb, feat), cols]
                    if i + j and not afar:
                        continue
                    if i + j:
                        remote(src, dst, gs_sem.at[own], gr_sem.at[own], at(z, y2, c2)).start()
                    else:
                        pltpu.make_async_copy(src, dst, gl_sem.at[own]).start()

    for r in range(chunks):
        turn(tp, r)
        share(tp, r * CHUNK, (r + 1) * CHUNK, 0)

    pltpu.make_async_copy(wcat, wcat, w_sem).wait()

    @pl.loop(0, pairs)
    def _(p):
        zacc[p, :rows, :] = dot32(
            xw[:, aligned(tp, dloc)], wcat[aligned(tp, dloc), aligned(p, TRIO)], ((1,), (0,))
        )

    @pl.when(sp == 0)
    def _():
        k_ext[:, :HALO, :] = jnp.zeros((pairs, HALO, LANES), BF)
        v_ext[:, :HALO, :] = jnp.zeros((pairs, HALO, LANES), BF)

    spot = lax.broadcasted_iota(jnp.int32, (rel_ref.shape[1], LINE), 1)
    entry = lax.broadcasted_iota(jnp.int32, (rel_ref.shape[1], LINE), 0)
    apart = jnp.where(spot < QB, spot, spot - LINE)
    picked = exact(rel_ref[...], jnp.where(bias_index(apart) == entry, 1.0, 0.0), ((1,), (0,)))
    for n in range(2 * pairs):
        lines[n] = picked[n : n + 1, :]

    def halo_copy(ref, n):
        return remote(
            ref.at[:, rows : rows + HALO, :], ref.at[:, :HALO, :],
            ks_sem.at[n], kr_sem.at[n], ahead,
        )

    def cross_copy(k, g):
        cols = pl.ds(pl.multiple_of(mod(mine + g, group) * rows, rows), rows - HALO)
        view = xg.at[aligned(tp, zparts * feat), cols]
        return remote(view, view, gs_sem.at[2], gr_sem.at[2], (sp, mod(tp + k, tps)))

    def project(p, r):
        part = slice(r * CHUNK, (r + 1) * CHUNK)
        total = zacc[p, part, :]
        for k in range(1, tps):
            t = mod(tp - k, tps)
            whole = xl[k - 1] if r == order[-1] else xw[part, aligned(t, dloc)]
            total = total + dot32(
                whole, wcat[aligned(t, dloc), aligned(p, TRIO)], ((1,), (0,))
            )
        low = total.astype(BF)
        q_s[p, part, :] = low[:, :LANES]
        k_ext[p, HALO + r * CHUNK : HALO + (r + 1) * CHUNK, :] = low[:, LANES : 2 * LANES]
        v_ext[p, HALO + r * CHUNK : HALO + (r + 1) * CHUNK, :] = low[:, 2 * LANES :]

    early = chunks - first - 1
    for n, r in enumerate(order):
        for k in range(1, tps):
            x_copy(k, r).wait_recv()

        if n == chunks - 1:
            some = xg.at[: zparts * feat, : (group - 1) * rows]
            pltpu.make_async_copy(some, some, gr_sem.at[0]).wait()
            some = xg.at[: zparts * feat, :rows]
            pltpu.make_async_copy(some, some, gl_sem.at[0]).wait()
            for k in range(1, tps):
                for g in range(1, group):
                    cross_copy(k, g).start()

        if n < chunks - 1:
            @pl.loop(0, pairs)
            def _(p):
                project(p, r)

        if n == early:
            @pl.when(has_ahead)
            def _():
                halo_copy(k_ext, 0).start()
                halo_copy(v_ext, 1).start()

        for k in range(1, tps):
            t = mod(tp - k, tps)
            if n < chunks - 1:
                turn(t, r)
            if n == min(early + 1, chunks - 1):
                for done in order[: early + 1]:
                    share(t, done * CHUNK, (done + 1) * CHUNK, 1)
            if early < n < chunks - 1:
                share(t, r * CHUNK, (r + 1) * CHUNK, 1, afar=False)

    pltpu.make_async_copy(d_s, d_s, d_sem).wait()

    @pl.when(has_behind)
    def _():
        halo_copy(k_ext, 0).wait_recv()
        halo_copy(v_ext, 1).wait_recv()

    key_row = lax.broadcasted_iota(jnp.int32, (KB, QB), 0)
    query_row = lax.broadcasted_iota(jnp.int32, (KB, QB), 1)
    lane = lax.broadcasted_iota(jnp.int32, (QB, LANES), 1)
    scale = HEAD ** (-0.5)
    zero = jnp.zeros((QB, LANES), BF)
    own_rows = aligned(mine, rows)

    def stacked(part):
        return jnp.concatenate(
            [jnp.where(lane < HEAD, part, zero), jnp.where(lane < HEAD, zero, part)], axis=0
        )

    def grad_halo(p):
        return remote(halo_s.at[p], halo_r.at[p], hs_sem, hr_sem.at[p], behind)

    def to_wide(p, m, k):
        view = alls[m].at[p, own_rows, :]
        return remote(
            view, view, ys_sem.at[m, k - 1], yr_sem.at[m, p, k - 1],
            at(z, mod(y + k, wide), core),
        )

    def to_mate(p, m, k):
        owner = aligned(mod(y - k, wide) * 2 + core, rows)
        view = alls[m].at[p, owner, :]
        return remote(view, view, cs_sem.at[m, k], cr_sem.at[m, p, k], mate)

    def spread_out(p, m):
        for k in range(1, wide):
            to_wide(p, m, k).start()
        to_mate(p, m, 0).start()

    def attend(p, between):
        project(p, order[-1])
        slot = lax.rem(p, 2)
        offset = key_row - jnp.where(query_row < SEG, 0, SEG)
        seen = (offset >= 0) & (offset < HALO + SEG)
        for half in range(2):
            line = jnp.broadcast_to(lines[2 * p + half], (KB, LINE))
            skewed = pltpu.roll(line, 0, 1, stride=1, stride_axis=0)[:, :QB]
            bias[:, half * QB : (half + 1) * QB] = jnp.where(seen, skewed, UNSEEN)
        kacc[slot] = jnp.zeros((ext, LANES), F32)
        vacc[slot] = jnp.zeros((ext, LANES), F32)
        bias_sum[...] = jnp.zeros_like(bias_sum)
        for block in range(blocks):
            keys = slice(block * QB, block * QB + KB)
            part = slice(block * QB, (block + 1) * QB)
            q2 = stacked(q_s[p, part, :] * BF(scale))
            d2 = stacked(d_s[p, part, :])
            k = k_ext[p, keys, :]
            v = v_ext[p, keys, :]
            score = dot32(k, q2, ((1,), (1,))) + bias[...]
            if block * QB < HALO:
                row = lax.broadcasted_iota(jnp.int32, (KB, 1), 0) + block * QB
                score = score + jnp.where((row < HALO) & (sp == 0), UNSEEN, 0.0)
            top = jnp.max(score, axis=0, keepdims=True)
            power = jnp.exp(score - top)
            prob = power * (1.0 / jnp.sum(power, axis=0, keepdims=True))
            prob_low = prob.astype(BF)
            grad_prob = dot32(v, d2, ((1,), (1,)))
            delta = jnp.sum(prob_low.astype(F32) * grad_prob, axis=0, keepdims=True)
            dscore = prob * (grad_prob - delta)
            bias_sum[...] += dscore
            dscore_low = dscore.astype(BF)
            vacc[slot, keys, :] += dot32(prob_low, d2, ((1,), (0,)))
            kacc[slot, keys, :] += dot32(dscore_low, q2, ((1,), (0,)))
            dq_t = dot32(k, dscore_low, ((0,), (0,)))
            dq_t = jnp.concatenate([dq_t[:HEAD, :QB], dq_t[HEAD:, QB:]], axis=0)
            dq = (dq_t.T * scale).astype(BF)
            xw[part, aligned(p * 3, LANES)] = dq
            all_q[p, pl.ds(pl.multiple_of(mine * rows + block * QB, QB), QB), :] = dq
            if block == HALO // QB - 1:
                halo_s[p, 0] = kacc[slot, :HALO, :].astype(BF)
                halo_s[p, 1] = vacc[slot, :HALO, :].astype(BF)

                @pl.when(has_behind)
                def _():
                    grad_halo(p).start()

                between()

        flip_row = lax.broadcasted_iota(jnp.int32, (KB, KB), 0)
        flip_col = lax.broadcasted_iota(jnp.int32, (KB, KB), 1)
        flip = jnp.where(flip_row + flip_col == KB - 1, 1.0, 0.0)
        flipped = exact(flip, bias_sum[...], ((1,), (0,)))
        for half in range(2):
            part = flipped[:, half * QB : (half + 1) * QB]
            spread = jnp.concatenate([part, jnp.zeros((KB, LINE - QB), F32)], axis=1)
            skewed = pltpu.roll(spread, 0, 1, stride=1, stride_axis=0)
            dline[2 * p + half] = jnp.sum(skewed, axis=0, keepdims=True)

    def settle(p):
        slot = lax.rem(p, 2)

        @pl.when(has_ahead)
        def _():
            grad_halo(p).wait_recv()
            kacc[slot, rows:, :] += halo_r[p, 0].astype(F32)
            vacc[slot, rows:, :] += halo_r[p, 1].astype(F32)

        for j, total in ((1, kacc), (2, vacc)):
            low = total[slot, HALO:, :].astype(BF)
            xw[:, aligned(p * 3 + j, LANES)] = low
            all_kv[p, own_rows, (j - 1) * LANES : j * LANES] = low

    def block_of(b):
        return slice(b * feat, (b + 1) * feat)

    def to_right(p, m, b):
        view = rights[m].at[p, b]
        return remote(view, view, rs_sem.at[m], rv_sem.at[m, p, b - 1], at(z + 1, y, core))

    def to_left(p, m, b):
        view = lefts[m].at[p, b]
        return remote(view, view, ls_sem.at[m], lv_sem.at[m, p, b], at(z - 1, y, core))

    def hop(p, m, h):
        @pl.when(z == h)
        def _():
            for b in range(deep - 1, h, -1):
                total = zacc[p, block_of(b), lanes[m]]
                if h:
                    to_right(p, m, b).wait_recv()
                    total = total + rights[m][p, b].astype(F32)
                rights[m][p, b] = total.astype(BF)
                to_right(p, m, b).start()

        @pl.when(z == deep - 1 - h)
        def _():
            for b in range(0, deep - 1 - h):
                total = zacc[p, block_of(b), lanes[m]]
                if h:
                    to_left(p, m, b).wait_recv()
                    total = total + lefts[m][p, b].astype(F32)
                lefts[m][p, b] = total.astype(BF)
                to_left(p, m, b).start()

    def forward(p, m):
        for k in range(1, wide):
            to_wide(p, m, k).wait_recv()
            to_mate(p, m, k).start()

    def product(p, m):
        if m == 0:
            @pl.when(p == 0)
            def _():
                others = slice(0, (deep - zparts) * feat)
                some = xg.at[others, : (group - 1) * HALO]
                pltpu.make_async_copy(some, some, gr_sem.at[1]).wait()
                some = xg.at[others, :rows]
                pltpu.make_async_copy(some, some, gl_sem.at[1]).wait()
                some = xg.at[others, : (group - 1) * (rows - HALO)]
                pltpu.make_async_copy(some, some, gr_sem.at[2]).wait()

        for k in range(wide):
            to_mate(p, m, k).wait_recv()
        zacc[p, : deep * feat, lanes[m]] = dot32(xg[...], alls[m][p], ((1,), (0,)))
        hop(p, m, 0)

    def grad_out(p, j):
        cols = aligned(p, LANES)
        return pltpu.make_async_copy(dw_ref.at[j, :, cols], dw_out.at[j, :, cols], o_sem.at[0])

    def finish(p, m):
        me = aligned(z, feat)

        @pl.when(z > 0)
        def _():
            to_right(p, m, z).wait_recv()
            zacc[p, me, lanes[m]] += rights[m][p, z].astype(F32)

        @pl.when(z < deep - 1)
        def _():
            to_left(p, m, z).wait_recv()
            zacc[p, me, lanes[m]] += lefts[m][p, z].astype(F32)

        total = zacc[p, me, lanes[m]]
        for j in range(1 + m):
            dw_ref[m + j, :, aligned(p, LANES)] = total[:, j * LANES : (j + 1) * LANES]
            grad_out(p, m + j).start()

    def near_copy(j, i):
        view = near.at[mine]
        return remote(
            view, view, bs_sem.at[0], br_sem.at[0], at(z, mod(y + j, wide), mod(core + i, 2))
        )

    def far_copy(k):
        view = far.at[z]
        return remote(view, view, bs_sem.at[1], br_sem.at[1], at(mod(z + k, deep), y, core))

    mates = [(j, i) for j in range(wide) for i in range(2) if i + j]

    def bias_near():
        near[mine] = jnp.concatenate([dline[n] for n in range(2 * pairs)], axis=0)
        for j, i in mates:
            near_copy(j, i).start()

    def bias_far():
        some = near.at[: group - 1]
        pltpu.make_async_copy(some, some, br_sem.at[0]).wait()
        total = near[0]
        for n in range(1, group):
            total = total + near[n]
        far[z] = total
        for k in range(1, deep):
            far_copy(k).start()

    tiles = dloc // TILE
    away = (tps - 1) * tiles

    def px_copy(j):
        return remote(
            pxs.at[j], pxr.at[j], ps_sem, pr_sem, (sp, mod(tp + 1 + lax.div(j, tiles), tps))
        )

    def input_tile(j):
        place = mod(tp + 1 + lax.div(j, tiles), tps) * tiles + lax.rem(j, tiles)
        low = dot32(
            xw[:, : pairs * TRIO], wcat[aligned(place, TILE), :], ((1,), (1,))
        ).astype(BF)

        @pl.when(j < away)
        def _():
            pxs[j] = low
            px_copy(j).start()

        @pl.when(j >= away)
        def _():
            gi_ref[:, aligned(j - away, TILE)] = low

    def bias_end():
        some = far.at[: deep - 1]
        pltpu.make_async_copy(some, some, br_sem.at[1]).wait()
        summed = far[0]
        for n in range(1, deep):
            summed = summed + far[n]
        spot = lax.broadcasted_iota(jnp.int32, (rel_ref.shape[1], LINE), 1)
        back = bias_index(spot - (KB - 1))
        entry = lax.broadcasted_iota(jnp.int32, (rel_ref.shape[1], LINE), 0)
        gb_ref[...] = exact(summed, jnp.where(back == entry, 1.0, 0.0), ((1,), (1,)))
        pltpu.make_async_copy(gb_ref, gb_out, o_sem.at[2]).start()

    def inputs_end():
        pltpu.make_async_copy(pxr, pxr, pr_sem).wait()
        for n in range(tiles):
            cols = slice(n * TILE, (n + 1) * TILE)
            total = gi_ref[:, cols].astype(F32)
            for k in range(1, tps):
                total = total + pxr[(k - 1) * tiles + n].astype(F32)
            gi_ref[:, cols] = total.astype(BF)
            pltpu.make_async_copy(gi_ref.at[:, cols], gi_out.at[:, cols], o_sem.at[1]).start()

    def first_sends():
        for r in order:
            for k in range(1, tps):
                x_copy(k, r).wait_send()
        some = xg.at[: zparts * feat, : (group - 1) * rows]
        pltpu.make_async_copy(some, some, gs_sem.at[0]).wait()
        some = xg.at[: (deep - zparts) * feat, : (group - 1) * HALO]
        pltpu.make_async_copy(some, some, gs_sem.at[1]).wait()
        some = xg.at[: (deep - zparts) * feat, : (group - 1) * (rows - HALO)]
        pltpu.make_async_copy(some, some, gs_sem.at[2]).wait()

        @pl.when(has_ahead)
        def _():
            halo_copy(k_ext, 0).wait_send()
            halo_copy(v_ext, 1).wait_send()

    hops = deep - 2
    early_pieces = pairs - 1
    last = 5 + hops
    rounds = 2 * pairs + last
    per = 2

    def staged(i, lag, stage):
        p = i - lag

        @pl.when((p >= 0) & (p < pairs))
        def _():
            stage(p)

    def pieced(i, lag, stage):
        piece = i - lag
        valid = (piece >= 0) & (piece < 2 * pairs)
        mixed = piece < early_pieces
        kv_left = pairs - early_pieces // 2
        parity = lax.rem(piece + 2 * last, 2)
        is_kv = jnp.where(mixed, parity, jnp.where(piece < early_pieces + kv_left, 1, 0))
        late_pair = jnp.where(is_kv == 1, piece - early_pieces + early_pieces // 2, piece - pairs)
        pair = jnp.where(mixed, lax.div(piece, 2), late_pair)
        for m in range(2):
            @pl.when(valid & (is_kv == m))
            def _():
                stage(pair, m)

    @pl.loop(0, rounds)
    def _(i):
        staged(i, 0, functools.partial(attend, between=lambda: pieced(i, 3, product)))

        @pl.when(i == pairs - 1)
        def _():
            bias_near()

        for lag in (1, 2):
            @pl.when((i < pairs) if lag == 1 else (i == pairs + 1))
            def _():
                staged(i, lag, settle)
        for m in range(2):
            @pl.when((i < early_pieces) & (lax.rem(i, 2) == m))
            def _():
                spread_out(lax.div(i, 2), m)

        @pl.when(i == 0)
        def _():
            for k in range(1, tps):
                r = order[-1]
                turn(mod(tp - k, tps), r, k - 1)
                share(mod(tp - k, tps), r * CHUNK, (r + 1) * CHUNK, 1, afar=False)

        @pl.when(i == pairs - 1)
        def _():
            for p in range(early_pieces // 2, pairs - 1):
                spread_out(p, 1)

        @pl.when(i == pairs + 1)
        def _():
            spread_out(pairs - 1, 1)
            for p in range((early_pieces + 1) // 2, pairs):
                spread_out(p, 0)

        @pl.when(i >= pairs)
        def _():
            pieced(i, 3, product)

        for h in range(1, hops + 1):
            pieced(i, 3 + h, functools.partial(hop, h=h))
        pieced(i, last, finish)
        pieced(i, 2, forward)

        @pl.when(i == pairs + 2)
        def _():
            first_sends()

        @pl.when(i == rounds - 3)
        def _():
            inputs_end()

        @pl.when(i == rounds - 2)
        def _():
            bias_end()

        @pl.when(i == pairs + 3)
        def _():
            bias_far()

        @pl.when(i > pairs)
        def _():
            @pl.loop(0, per)
            def _(n):
                j = (i - pairs - 1) * per + n

                @pl.when(j < tps * tiles)
                def _():
                    input_tile(j)

    pltpu.make_async_copy(pxs, pxs, ps_sem).wait()
    for m in range(2):
        for zi in range(deep):
            @pl.when(z == zi)
            def _():
                if zi < deep - 1:
                    some = rights[m].at[:, : deep - 1 - zi]
                    pltpu.make_async_copy(some, some, rs_sem.at[m]).wait()
                if zi:
                    some = lefts[m].at[:, :zi]
                    pltpu.make_async_copy(some, some, ls_sem.at[m]).wait()
        some = alls[m].at[:, :rows]
        for k in range(1, wide):
            pltpu.make_async_copy(some, some, ys_sem.at[m, k - 1]).wait()
        for k in range(wide):
            pltpu.make_async_copy(some, some, cs_sem.at[m, k]).wait()

    @pl.when(has_behind)
    def _():
        pltpu.make_async_copy(halo_s, halo_s, hs_sem).wait()

    for j, i in mates:
        near_copy(j, i).wait_send()
    for k in range(1, deep):
        far_copy(k).wait_send()
    pltpu.make_async_copy(gi_ref, gi_out, o_sem.at[1]).wait()
    pltpu.make_async_copy(gb_ref, gb_out, o_sem.at[2]).wait()
    pltpu.make_async_copy(dw_ref, dw_out, o_sem.at[0]).wait()


def hand_body(gi, dw, gb, gi_out, dwq_out, dwk_out, dwv_out, gb_out, gi_v, dw_v, gb_v, i_sem, o_sem):
    outs = (dwq_out, dwk_out, dwv_out)
    rows = gi.shape[0] // 2
    moves = [(gi.at[n * rows : (n + 1) * rows], gi_v.at[n * rows : (n + 1) * rows],
              gi_out.at[n * rows : (n + 1) * rows]) for n in range(2)]
    moves += [(dw.at[j], dw_v.at[j], outs[j]) for j in range(3)]
    moves.append((gb, gb_v, gb_out))
    for n, (src, mid, _) in enumerate(moves):
        pltpu.make_async_copy(src, mid, i_sem.at[n]).start()
    for n, (src, mid, dst) in enumerate(moves):
        pltpu.make_async_copy(src, mid, i_sem.at[n]).wait()
        pltpu.make_async_copy(mid, dst, o_sem.at[n]).start()
    for n, (_, mid, dst) in enumerate(moves):
        pltpu.make_async_copy(mid, dst, o_sem.at[n]).wait()


def local(sizes, inputs, w_query, w_key, w_value, rel_bias, d_out):
    seq, tps = sizes
    deep, wide = grid_of(seq // 2)
    rows, dloc = inputs.shape
    full, width = w_query.shape
    pairs = width // LANES
    ext = HALO + rows
    feat = full // seq
    group = 2 * wide
    tiles = dloc // TILE
    chunks = rows // CHUNK
    heads = rel_bias.shape[1]
    sds = jax.ShapeDtypeStruct
    vm = pltpu.VMEM
    dma = pltpu.SemaphoreType.DMA
    hbm = pl.BlockSpec(memory_space=pl.ANY)
    on_chip = pl.BlockSpec(memory_space=pltpu.VMEM)
    out = pl.pallas_call(
        functools.partial(step_body, sizes),
        in_specs=[hbm, hbm, hbm, hbm, on_chip, hbm],
        out_specs=[hbm] * 3,
        out_shape=[
            sds((rows, dloc), BF),
            sds((3, feat, width), F32),
            sds((heads, rel_bias.shape[0]), F32),
        ],
        scratch_shapes=[
            vm((rows, full), BF),
            vm((full, pairs * TRIO), BF),
            vm((full, rows), BF),
            vm((deep * feat, group * rows), BF),
            vm((pairs, max(deep * feat, rows), TRIO), F32),
            vm((pairs, rows, LANES), BF),
            vm((pairs, ext, LANES), BF),
            vm((pairs, ext, LANES), BF),
            vm((pairs, rows, LANES), BF),
            vm((2 * pairs, 1, LINE), F32),
            vm((2 * pairs, 1, LINE), F32),
            vm((KB, 2 * QB), F32),
            vm((KB, 2 * QB), F32),
            vm((2, ext, LANES), F32),
            vm((2, ext, LANES), F32),
            vm((pairs, 2, HALO, LANES), BF),
            vm((pairs, 2, HALO, LANES), BF),
            vm((pairs, group * rows, LANES), BF),
            vm((pairs, group * rows, 2 * LANES), BF),
            vm((pairs, deep, feat, LANES), BF),
            vm((pairs, deep, feat, 2 * LANES), BF),
            vm((pairs, deep, feat, LANES), BF),
            vm((pairs, deep, feat, 2 * LANES), BF),
            vm(((tps - 1) * tiles, rows, TILE), BF),
            vm(((tps - 1) * tiles, rows, TILE), BF),
            vm((group, 2 * pairs, LINE), F32),
            vm((deep, 2 * pairs, LINE), F32),
            vm((tps - 1, CHUNK, dloc), BF),
            vm((rows, dloc), BF),
            vm((3, feat, width), F32),
            vm((heads, rel_bias.shape[0]), F32),
            dma((3,)),
            dma(()), dma(()), dma(()),
            dma((tps - 1, chunks)), dma((tps - 1, chunks)),
            dma((3,)), dma((3,)), dma((2,)),
            dma((2,)), dma((2,)),
            dma(()), dma((pairs,)),
            dma((2, wide - 1)), dma((2, pairs, wide - 1)),
            dma((2, wide)), dma((2, pairs, wide)),
            dma((2,)), dma((2, pairs, deep - 1)),
            dma((2,)), dma((2, pairs, deep - 1)),
            dma((2,)), dma((2,)),
            dma(()), dma(()),
        ],
        compiler_params=pltpu.CompilerParams(
            collective_id=0, has_side_effects=True, vmem_limit_bytes=67043328
        ),
        name="whole_step",
    )(inputs, w_query, w_key, w_value, rel_bias.T, d_out)
    grad = sds((feat, width), F32)
    out = pl.pallas_call(
        hand_body,
        in_specs=[hbm] * 3,
        out_specs=[hbm] * 5,
        out_shape=[sds((rows, dloc), BF), grad, grad, grad, sds((heads, rel_bias.shape[0]), F32)],
        scratch_shapes=[
            vm((rows, dloc), BF), vm((3, feat, width), F32), vm((heads, rel_bias.shape[0]), F32),
            dma((6,)), dma((6,)),
        ],
        name="hand_out",
    )(*out)
    return out[0], out[1], out[2], out[3], out[4].T


def solution(mesh):
    placed = (
        P("sp", "tp"),
        P(None, "tp"),
        P(None, "tp"),
        P(None, "tp"),
        P(None, "tp"),
        P("sp", "tp"),
    )
    sizes = (mesh.shape["sp"], mesh.shape["tp"])
    return jax.shard_map(
        functools.partial(local, sizes),
        mesh=mesh,
        in_specs=placed,
        out_specs=(P("sp", "tp"), P("sp", "tp"), P("sp", "tp"), P("sp", "tp"), P(None, "tp")),
        check_vma=False,
    )
```

```python
import functools

import jax
import jax.numpy as jnp
from jax import lax
from jax.experimental import pallas as pl
from jax.experimental.pallas import tpu as pltpu
from jax.sharding import PartitionSpec as P

HEAD = 64
SEG = 64
LEFT = 4
REL_MAX = 256
LANES = 128
QB = 2 * SEG
HALO = LEFT * SEG
KB = HALO + QB
LINE = 512
UNSEEN = -1e30
CHUNK = 128
TILE = 256
TRIO = 3 * LANES
MESH = pl.DeviceIdType.MESH
BF = jnp.bfloat16
F32 = jnp.float32


def dot32(a, b, dims):
    return lax.dot_general(a, b, (dims, ((), ())), preferred_element_type=F32)


def exact(a, b, dims):
    return lax.dot_general(
        a, b, (dims, ((), ())), precision=lax.Precision.HIGHEST, preferred_element_type=F32
    )


def grid_of(chips):
    depth = 1
    while depth * depth < chips:
        depth *= 2
    return depth, chips // depth


def aligned(index, size):
    return pl.ds(pl.multiple_of(index * size, size), size)


def bias_index(apart):
    return jnp.clip(HALO + apart, 1 - SEG, REL_MAX) + SEG - 1


def step_body(
    sizes,
    x_ref, wq_ref, wk_ref, wv_ref, rel_ref, d_ref,
    gi_out, dw_out, gb_out,
    xw, wcat, xt, xg, zacc, q_s, k_ext, v_ext, d_s, lines, dline, bias, bias_sum, kacc, vacc,
    halo_s, halo_r, all_q, all_kv, right_q, right_kv, left_q, left_kv, pxs, pxr, near, far,
    xl, gi_ref, dw_ref, gb_ref, o_sem,
    w_sem, d_sem, x_sem, xs_sem, xr_sem, gs_sem, gr_sem, gl_sem, ks_sem, kr_sem, hs_sem, hr_sem,
    ys_sem, yr_sem, cs_sem, cr_sem, rs_sem, rv_sem, ls_sem, lv_sem, bs_sem, br_sem, ps_sem, pr_sem,
):
    alls, rights, lefts = (all_q, all_kv), (right_q, right_kv), (left_q, left_kv)
    lanes = (slice(0, LANES), slice(LANES, TRIO))
    seq, tps = sizes
    deep, wide = grid_of(seq // 2)
    rows, dloc = x_ref.shape
    pairs = wq_ref.shape[1] // LANES
    ext = HALO + rows
    blocks = rows // QB
    feat = dloc * tps // seq
    group = 2 * wide
    sp = lax.axis_index("sp")
    tp = lax.axis_index("tp")
    core = lax.rem(sp, 2)
    chip = lax.div(sp, 2)
    y = lax.rem(chip, wide)
    z = lax.div(chip, wide)
    mine = y * 2 + core

    def at(zi, yi, ci):
        return ((zi * wide + yi) * 2 + ci, tp)

    def mod(a, n):
        return lax.rem(a + n, n)

    mate = at(z, y, 1 - core)
    ahead, behind = (sp + 1, tp), (sp - 1, tp)
    has_ahead, has_behind = sp + 1 < seq, sp > 0

    greeted = [(sp, mod(tp + k, tps)) for k in range(1, tps)]
    greeted += [(mod(sp + 1, seq), tp), (mod(sp - 1, seq), tp)]
    greeted += [at(z, mod(y + j, wide), mod(core + i, 2)) for j in range(wide) for i in range(2) if i + j]
    greeted += [at(mod(z + k, deep), y, core) for k in range(1, deep)]
    barrier = pltpu.get_barrier_semaphore()
    for other in greeted:
        pl.semaphore_signal(barrier, inc=1, device_id=other, device_id_type=MESH)

    own_x = pltpu.make_async_copy(x_ref, xw.at[:, aligned(tp, dloc)], x_sem)
    own_x.start()
    for p in range(pairs):
        for j, w_ref in enumerate((wq_ref, wk_ref, wv_ref)):
            pltpu.make_async_copy(
                w_ref.at[:, p * LANES : (p + 1) * LANES],
                wcat.at[:, p * TRIO + j * LANES : p * TRIO + (j + 1) * LANES], w_sem,
            ).start()
    for p in range(pairs):
        pltpu.make_async_copy(
            d_ref.at[:, p * LANES : (p + 1) * LANES], d_s.at[p], d_sem
        ).start()
    pl.semaphore_wait(barrier, len(greeted))

    def remote(src, dst, send, recv, device):
        return pltpu.make_async_remote_copy(
            src_ref=src, dst_ref=dst, send_sem=send, recv_sem=recv,
            device_id=device, device_id_type=MESH,
        )

    chunks = rows // CHUNK
    first = (rows - HALO) // CHUNK
    order = list(range(first, chunks)) + list(range(first))

    def x_copy(k, r):
        part = slice(r * CHUNK, (r + 1) * CHUNK)
        landing = xl.at[k - 1] if r == order[-1] else xw.at[part, aligned(tp, dloc)]
        return remote(
            x_ref.at[part, :], landing,
            xs_sem.at[k - 1, r], xr_sem.at[k - 1, r], (sp, mod(tp + k, tps)),
        )

    for r in order:
        for k in range(1, tps):
            x_copy(k, r).start()
    own_x.wait()

    def turn(t, r, source=None):
        part = slice(r * CHUNK, (r + 1) * CHUNK)

        @pl.loop(0, dloc // TILE)
        def _(f):
            cols = aligned(t * (dloc // TILE) + f, TILE)
            if source is None:
                xt[cols, part] = xw[part, cols].T
            else:
                xt[cols, part] = xl[source, :, aligned(f, TILE)].T

    zparts = deep // tps

    def share(t, low, high, own, afar=True):
        for j in range(wide):
            for i in range(2):
                for q in range(zparts):
                    zb = t * zparts + q
                    y2, c2 = mod(y + j, wide), mod(core + i, 2)
                    src = xt.at[aligned((zb * wide + y2) * 2 + c2, feat), low:high]
                    cols = pl.ds(pl.multiple_of(mine * rows + low, CHUNK), high - low)
                    dst = xg.at[aligned(zb, feat), cols]
                    if i + j and not afar:
                        continue
                    if i + j:
                        remote(src, dst, gs_sem.at[own], gr_sem.at[own], at(z, y2, c2)).start()
                    else:
                        pltpu.make_async_copy(src, dst, gl_sem.at[own]).start()

    for r in range(chunks):
        turn(tp, r)
        share(tp, r * CHUNK, (r + 1) * CHUNK, 0)

    pltpu.make_async_copy(wcat, wcat, w_sem).wait()

    @pl.loop(0, pairs)
    def _(p):
        zacc[p, :rows, :] = dot32(
            xw[:, aligned(tp, dloc)], wcat[aligned(tp, dloc), aligned(p, TRIO)], ((1,), (0,))
        )

    @pl.when(sp == 0)
    def _():
        k_ext[:, :HALO, :] = jnp.zeros((pairs, HALO, LANES), BF)
        v_ext[:, :HALO, :] = jnp.zeros((pairs, HALO, LANES), BF)

    spot = lax.broadcasted_iota(jnp.int32, (rel_ref.shape[1], LINE), 1)
    entry = lax.broadcasted_iota(jnp.int32, (rel_ref.shape[1], LINE), 0)
    apart = jnp.where(spot < QB, spot, spot - LINE)
    picked = exact(rel_ref[...], jnp.where(bias_index(apart) == entry, 1.0, 0.0), ((1,), (0,)))
    for n in range(2 * pairs):
        lines[n] = picked[n : n + 1, :]

    def halo_copy(ref, n):
        return remote(
            ref.at[:, rows : rows + HALO, :], ref.at[:, :HALO, :],
            ks_sem.at[n], kr_sem.at[n], ahead,
        )

    def cross_copy(k, g):
        cols = pl.ds(pl.multiple_of(mod(mine + g, group) * rows, rows), rows - HALO)
        view = xg.at[aligned(tp, zparts * feat), cols]
        return remote(view, view, gs_sem.at[2], gr_sem.at[2], (sp, mod(tp + k, tps)))

    def project(p, r):
        part = slice(r * CHUNK, (r + 1) * CHUNK)
        total = zacc[p, part, :]
        for k in range(1, tps):
            t = mod(tp - k, tps)
            whole = xl[k - 1] if r == order[-1] else xw[part, aligned(t, dloc)]
            total = total + dot32(
                whole, wcat[aligned(t, dloc), aligned(p, TRIO)], ((1,), (0,))
            )
        low = total.astype(BF)
        q_s[p, part, :] = low[:, :LANES]
        k_ext[p, HALO + r * CHUNK : HALO + (r + 1) * CHUNK, :] = low[:, LANES : 2 * LANES]
        v_ext[p, HALO + r * CHUNK : HALO + (r + 1) * CHUNK, :] = low[:, 2 * LANES :]

    early = chunks - first - 1
    for n, r in enumerate(order):
        for k in range(1, tps):
            x_copy(k, r).wait_recv()

        if n == chunks - 1:
            some = xg.at[: zparts * feat, : (group - 1) * rows]
            pltpu.make_async_copy(some, some, gr_sem.at[0]).wait()
            some = xg.at[: zparts * feat, :rows]
            pltpu.make_async_copy(some, some, gl_sem.at[0]).wait()
            for k in range(1, tps):
                for g in range(1, group):
                    cross_copy(k, g).start()

        if n < chunks - 1:
            @pl.loop(0, pairs)
            def _(p):
                project(p, r)

        if n == early:
            @pl.when(has_ahead)
            def _():
                halo_copy(k_ext, 0).start()
                halo_copy(v_ext, 1).start()

        for k in range(1, tps):
            t = mod(tp - k, tps)
            if n < chunks - 1:
                turn(t, r)
            if n == min(early + 1, chunks - 1):
                for done in order[: early + 1]:
                    share(t, done * CHUNK, (done + 1) * CHUNK, 1)
            if early < n < chunks - 1:
                share(t, r * CHUNK, (r + 1) * CHUNK, 1, afar=False)

    pltpu.make_async_copy(d_s, d_s, d_sem).wait()

    @pl.when(has_behind)
    def _():
        halo_copy(k_ext, 0).wait_recv()
        halo_copy(v_ext, 1).wait_recv()

    key_row = lax.broadcasted_iota(jnp.int32, (KB, QB), 0)
    query_row = lax.broadcasted_iota(jnp.int32, (KB, QB), 1)
    lane = lax.broadcasted_iota(jnp.int32, (QB, LANES), 1)
    scale = HEAD ** (-0.5)
    zero = jnp.zeros((QB, LANES), BF)
    own_rows = aligned(mine, rows)

    def stacked(part):
        return jnp.concatenate(
            [jnp.where(lane < HEAD, part, zero), jnp.where(lane < HEAD, zero, part)], axis=0
        )

    def grad_halo(p):
        return remote(halo_s.at[p], halo_r.at[p], hs_sem, hr_sem.at[p], behind)

    def to_wide(p, m, k):
        view = alls[m].at[p, own_rows, :]
        return remote(
            view, view, ys_sem.at[m, k - 1], yr_sem.at[m, p, k - 1],
            at(z, mod(y + k, wide), core),
        )

    def to_mate(p, m, k):
        owner = aligned(mod(y - k, wide) * 2 + core, rows)
        view = alls[m].at[p, owner, :]
        return remote(view, view, cs_sem.at[m, k], cr_sem.at[m, p, k], mate)

    def spread_out(p, m):
        for k in range(1, wide):
            to_wide(p, m, k).start()
        to_mate(p, m, 0).start()

    def attend(p, between):
        project(p, order[-1])
        slot = lax.rem(p, 2)
        offset = key_row - jnp.where(query_row < SEG, 0, SEG)
        seen = (offset >= 0) & (offset < HALO + SEG)
        for half in range(2):
            line = jnp.broadcast_to(lines[2 * p + half], (KB, LINE))
            skewed = pltpu.roll(line, 0, 1, stride=1, stride_axis=0)[:, :QB]
            bias[:, half * QB : (half + 1) * QB] = jnp.where(seen, skewed, UNSEEN)
        kacc[slot] = jnp.zeros((ext, LANES), F32)
        vacc[slot] = jnp.zeros((ext, LANES), F32)
        bias_sum[...] = jnp.zeros_like(bias_sum)
        for block in range(blocks):
            keys = slice(block * QB, block * QB + KB)
            part = slice(block * QB, (block + 1) * QB)
            q2 = stacked(q_s[p, part, :] * BF(scale))
            d2 = stacked(d_s[p, part, :])
            k = k_ext[p, keys, :]
            v = v_ext[p, keys, :]
            score = dot32(k, q2, ((1,), (1,))) + bias[...]
            if block * QB < HALO:
                row = lax.broadcasted_iota(jnp.int32, (KB, 1), 0) + block * QB
                score = score + jnp.where((row < HALO) & (sp == 0), UNSEEN, 0.0)
            top = jnp.max(score, axis=0, keepdims=True)
            power = jnp.exp(score - top)
            prob = power * (1.0 / jnp.sum(power, axis=0, keepdims=True))
            prob_low = prob.astype(BF)
            grad_prob = dot32(v, d2, ((1,), (1,)))
            delta = jnp.sum(prob_low.astype(F32) * grad_prob, axis=0, keepdims=True)
            dscore = prob * (grad_prob - delta)
            bias_sum[...] += dscore
            dscore_low = dscore.astype(BF)
            vacc[slot, keys, :] += dot32(prob_low, d2, ((1,), (0,)))
            kacc[slot, keys, :] += dot32(dscore_low, q2, ((1,), (0,)))
            dq_t = dot32(k, dscore_low, ((0,), (0,)))
            dq_t = jnp.concatenate([dq_t[:HEAD, :QB], dq_t[HEAD:, QB:]], axis=0)
            dq = (dq_t.T * scale).astype(BF)
            xw[part, aligned(p * 3, LANES)] = dq
            all_q[p, pl.ds(pl.multiple_of(mine * rows + block * QB, QB), QB), :] = dq
            if block == HALO // QB - 1:
                halo_s[p, 0] = kacc[slot, :HALO, :].astype(BF)
                halo_s[p, 1] = vacc[slot, :HALO, :].astype(BF)

                @pl.when(has_behind)
                def _():
                    grad_halo(p).start()

                between()

        flip_row = lax.broadcasted_iota(jnp.int32, (KB, KB), 0)
        flip_col = lax.broadcasted_iota(jnp.int32, (KB, KB), 1)
        flip = jnp.where(flip_row + flip_col == KB - 1, 1.0, 0.0)
        flipped = exact(flip, bias_sum[...], ((1,), (0,)))
        for half in range(2):
            part = flipped[:, half * QB : (half + 1) * QB]
            spread = jnp.concatenate([part, jnp.zeros((KB, LINE - QB), F32)], axis=1)
            skewed = pltpu.roll(spread, 0, 1, stride=1, stride_axis=0)
            dline[2 * p + half] = jnp.sum(skewed, axis=0, keepdims=True)

    def settle(p):
        slot = lax.rem(p, 2)

        @pl.when(has_ahead)
        def _():
            grad_halo(p).wait_recv()
            kacc[slot, rows:, :] += halo_r[p, 0].astype(F32)
            vacc[slot, rows:, :] += halo_r[p, 1].astype(F32)

        for j, total in ((1, kacc), (2, vacc)):
            low = total[slot, HALO:, :].astype(BF)
            xw[:, aligned(p * 3 + j, LANES)] = low
            all_kv[p, own_rows, (j - 1) * LANES : j * LANES] = low

    def block_of(b):
        return slice(b * feat, (b + 1) * feat)

    def to_right(p, m, b):
        view = rights[m].at[p, b]
        return remote(view, view, rs_sem.at[m], rv_sem.at[m, p, b - 1], at(z + 1, y, core))

    def to_left(p, m, b):
        view = lefts[m].at[p, b]
        return remote(view, view, ls_sem.at[m], lv_sem.at[m, p, b], at(z - 1, y, core))

    def hop(p, m, h):
        @pl.when(z == h)
        def _():
            for b in range(deep - 1, h, -1):
                total = zacc[p, block_of(b), lanes[m]]
                if h:
                    to_right(p, m, b).wait_recv()
                    total = total + rights[m][p, b].astype(F32)
                rights[m][p, b] = total.astype(BF)
                to_right(p, m, b).start()

        @pl.when(z == deep - 1 - h)
        def _():
            for b in range(0, deep - 1 - h):
                total = zacc[p, block_of(b), lanes[m]]
                if h:
                    to_left(p, m, b).wait_recv()
                    total = total + lefts[m][p, b].astype(F32)
                lefts[m][p, b] = total.astype(BF)
                to_left(p, m, b).start()

    def forward(p, m):
        for k in range(1, wide):
            to_wide(p, m, k).wait_recv()
            to_mate(p, m, k).start()

    def product(p, m):
        if m == 0:
            @pl.when(p == 0)
            def _():
                others = slice(0, (deep - zparts) * feat)
                some = xg.at[others, : (group - 1) * HALO]
                pltpu.make_async_copy(some, some, gr_sem.at[1]).wait()
                some = xg.at[others, :rows]
                pltpu.make_async_copy(some, some, gl_sem.at[1]).wait()
                some = xg.at[others, : (group - 1) * (rows - HALO)]
                pltpu.make_async_copy(some, some, gr_sem.at[2]).wait()

        for k in range(wide):
            to_mate(p, m, k).wait_recv()
        zacc[p, : deep * feat, lanes[m]] = dot32(xg[...], alls[m][p], ((1,), (0,)))
        hop(p, m, 0)

    def grad_out(p, j):
        cols = aligned(p, LANES)
        return pltpu.make_async_copy(dw_ref.at[j, :, cols], dw_out.at[j, :, cols], o_sem.at[0])

    def finish(p, m):
        me = aligned(z, feat)

        @pl.when(z > 0)
        def _():
            to_right(p, m, z).wait_recv()
            zacc[p, me, lanes[m]] += rights[m][p, z].astype(F32)

        @pl.when(z < deep - 1)
        def _():
            to_left(p, m, z).wait_recv()
            zacc[p, me, lanes[m]] += lefts[m][p, z].astype(F32)

        total = zacc[p, me, lanes[m]]
        for j in range(1 + m):
            dw_ref[m + j, :, aligned(p, LANES)] = total[:, j * LANES : (j + 1) * LANES]
            grad_out(p, m + j).start()

    def near_copy(j, i):
        view = near.at[mine]
        return remote(
            view, view, bs_sem.at[0], br_sem.at[0], at(z, mod(y + j, wide), mod(core + i, 2))
        )

    def far_copy(k):
        view = far.at[z]
        return remote(view, view, bs_sem.at[1], br_sem.at[1], at(mod(z + k, deep), y, core))

    mates = [(j, i) for j in range(wide) for i in range(2) if i + j]

    def bias_near():
        near[mine] = jnp.concatenate([dline[n] for n in range(2 * pairs)], axis=0)
        for j, i in mates:
            near_copy(j, i).start()

    def bias_far():
        some = near.at[: group - 1]
        pltpu.make_async_copy(some, some, br_sem.at[0]).wait()
        total = near[0]
        for n in range(1, group):
            total = total + near[n]
        far[z] = total
        for k in range(1, deep):
            far_copy(k).start()

    tiles = dloc // TILE
    away = (tps - 1) * tiles

    def px_copy(j):
        return remote(
            pxs.at[j], pxr.at[j], ps_sem, pr_sem, (sp, mod(tp + 1 + lax.div(j, tiles), tps))
        )

    def input_tile(j):
        place = mod(tp + 1 + lax.div(j, tiles), tps) * tiles + lax.rem(j, tiles)
        low = dot32(
            xw[:, : pairs * TRIO], wcat[aligned(place, TILE), :], ((1,), (1,))
        ).astype(BF)

        @pl.when(j < away)
        def _():
            pxs[j] = low
            px_copy(j).start()

        @pl.when(j >= away)
        def _():
            gi_ref[:, aligned(j - away, TILE)] = low

    def bias_end():
        some = far.at[: deep - 1]
        pltpu.make_async_copy(some, some, br_sem.at[1]).wait()
        summed = far[0]
        for n in range(1, deep):
            summed = summed + far[n]
        spot = lax.broadcasted_iota(jnp.int32, (rel_ref.shape[1], LINE), 1)
        back = bias_index(spot - (KB - 1))
        entry = lax.broadcasted_iota(jnp.int32, (rel_ref.shape[1], LINE), 0)
        gb_ref[...] = exact(summed, jnp.where(back == entry, 1.0, 0.0), ((1,), (1,)))
        pltpu.make_async_copy(gb_ref, gb_out, o_sem.at[2]).start()

    def inputs_end():
        pltpu.make_async_copy(pxr, pxr, pr_sem).wait()
        for n in range(tiles):
            cols = slice(n * TILE, (n + 1) * TILE)
            total = gi_ref[:, cols].astype(F32)
            for k in range(1, tps):
                total = total + pxr[(k - 1) * tiles + n].astype(F32)
            gi_ref[:, cols] = total.astype(BF)
            pltpu.make_async_copy(gi_ref.at[:, cols], gi_out.at[:, cols], o_sem.at[1]).start()

    def first_sends():
        for r in order:
            for k in range(1, tps):
                x_copy(k, r).wait_send()
        some = xg.at[: zparts * feat, : (group - 1) * rows]
        pltpu.make_async_copy(some, some, gs_sem.at[0]).wait()
        some = xg.at[: (deep - zparts) * feat, : (group - 1) * HALO]
        pltpu.make_async_copy(some, some, gs_sem.at[1]).wait()
        some = xg.at[: (deep - zparts) * feat, : (group - 1) * (rows - HALO)]
        pltpu.make_async_copy(some, some, gs_sem.at[2]).wait()

        @pl.when(has_ahead)
        def _():
            halo_copy(k_ext, 0).wait_send()
            halo_copy(v_ext, 1).wait_send()

    hops = deep - 2
    early_pieces = max(pairs - 2, 1)
    last = 5 + hops
    rounds = 2 * pairs + last
    per = 2

    def staged(i, lag, stage):
        p = i - lag

        @pl.when((p >= 0) & (p < pairs))
        def _():
            stage(p)

    def pieced(i, lag, stage):
        piece = i - lag
        valid = (piece >= 0) & (piece < 2 * pairs)
        mixed = piece < early_pieces
        kv_left = pairs - early_pieces // 2
        parity = lax.rem(piece + 2 * last, 2)
        is_kv = jnp.where(mixed, parity, jnp.where(piece < early_pieces + kv_left, 1, 0))
        late_pair = jnp.where(is_kv == 1, piece - early_pieces + early_pieces // 2, piece - pairs)
        pair = jnp.where(mixed, lax.div(piece, 2), late_pair)
        for m in range(2):
            @pl.when(valid & (is_kv == m))
            def _():
                stage(pair, m)

    @pl.loop(0, rounds)
    def _(i):
        staged(i, 0, functools.partial(attend, between=lambda: pieced(i, 3, product)))

        @pl.when(i == pairs - 1)
        def _():
            bias_near()

        for lag in (1, 2):
            @pl.when((i < pairs) if lag == 1 else (i == pairs + 1))
            def _():
                staged(i, lag, settle)
        for m in range(2):
            @pl.when((i < early_pieces) & (lax.rem(i, 2) == m))
            def _():
                spread_out(lax.div(i, 2), m)

        @pl.when(i == 0)
        def _():
            for k in range(1, tps):
                r = order[-1]
                turn(mod(tp - k, tps), r, k - 1)
                share(mod(tp - k, tps), r * CHUNK, (r + 1) * CHUNK, 1, afar=False)

        @pl.when(i == pairs - 1)
        def _():
            for p in range(early_pieces // 2, pairs - 1):
                spread_out(p, 1)

        @pl.when(i == pairs + 1)
        def _():
            spread_out(pairs - 1, 1)
            for p in range((early_pieces + 1) // 2, pairs):
                spread_out(p, 0)

        @pl.when(i >= pairs)
        def _():
            pieced(i, 3, product)

        for h in range(1, hops + 1):
            pieced(i, 3 + h, functools.partial(hop, h=h))
        pieced(i, last, finish)
        pieced(i, 2, forward)

        @pl.when(i == pairs + 2)
        def _():
            first_sends()

        @pl.when(i == rounds - 3)
        def _():
            inputs_end()

        @pl.when(i == rounds - 2)
        def _():
            bias_end()

        @pl.when(i == pairs + 3)
        def _():
            bias_far()

        @pl.when(i > pairs)
        def _():
            @pl.loop(0, per)
            def _(n):
                j = (i - pairs - 1) * per + n

                @pl.when(j < tps * tiles)
                def _():
                    input_tile(j)

    pltpu.make_async_copy(pxs, pxs, ps_sem).wait()
    for m in range(2):
        for zi in range(deep):
            @pl.when(z == zi)
            def _():
                if zi < deep - 1:
                    some = rights[m].at[:, : deep - 1 - zi]
                    pltpu.make_async_copy(some, some, rs_sem.at[m]).wait()
                if zi:
                    some = lefts[m].at[:, :zi]
                    pltpu.make_async_copy(some, some, ls_sem.at[m]).wait()
        some = alls[m].at[:, :rows]
        for k in range(1, wide):
            pltpu.make_async_copy(some, some, ys_sem.at[m, k - 1]).wait()
        for k in range(wide):
            pltpu.make_async_copy(some, some, cs_sem.at[m, k]).wait()

    @pl.when(has_behind)
    def _():
        pltpu.make_async_copy(halo_s, halo_s, hs_sem).wait()

    for j, i in mates:
        near_copy(j, i).wait_send()
    for k in range(1, deep):
        far_copy(k).wait_send()
    pltpu.make_async_copy(gi_ref, gi_out, o_sem.at[1]).wait()
    pltpu.make_async_copy(gb_ref, gb_out, o_sem.at[2]).wait()
    pltpu.make_async_copy(dw_ref, dw_out, o_sem.at[0]).wait()


def hand_body(gi, dw, gb, gi_out, dwq_out, dwk_out, dwv_out, gb_out, gi_v, dw_v, gb_v, i_sem, o_sem):
    outs = (dwq_out, dwk_out, dwv_out)
    rows = gi.shape[0] // 2
    moves = [(gi.at[n * rows : (n + 1) * rows], gi_v.at[n * rows : (n + 1) * rows],
              gi_out.at[n * rows : (n + 1) * rows]) for n in range(2)]
    moves += [(dw.at[j], dw_v.at[j], outs[j]) for j in range(3)]
    moves.append((gb, gb_v, gb_out))
    for n, (src, mid, _) in enumerate(moves):
        pltpu.make_async_copy(src, mid, i_sem.at[n]).start()
    for n, (src, mid, dst) in enumerate(moves):
        pltpu.make_async_copy(src, mid, i_sem.at[n]).wait()
        pltpu.make_async_copy(mid, dst, o_sem.at[n]).start()
    for n, (_, mid, dst) in enumerate(moves):
        pltpu.make_async_copy(mid, dst, o_sem.at[n]).wait()


def local(sizes, inputs, w_query, w_key, w_value, rel_bias, d_out):
    seq, tps = sizes
    deep, wide = grid_of(seq // 2)
    rows, dloc = inputs.shape
    full, width = w_query.shape
    pairs = width // LANES
    ext = HALO + rows
    feat = full // seq
    group = 2 * wide
    tiles = dloc // TILE
    chunks = rows // CHUNK
    heads = rel_bias.shape[1]
    sds = jax.ShapeDtypeStruct
    vm = pltpu.VMEM
    dma = pltpu.SemaphoreType.DMA
    hbm = pl.BlockSpec(memory_space=pl.ANY)
    on_chip = pl.BlockSpec(memory_space=pltpu.VMEM)
    out = pl.pallas_call(
        functools.partial(step_body, sizes),
        in_specs=[hbm, hbm, hbm, hbm, on_chip, hbm],
        out_specs=[hbm] * 3,
        out_shape=[
            sds((rows, dloc), BF),
            sds((3, feat, width), F32),
            sds((heads, rel_bias.shape[0]), F32),
        ],
        scratch_shapes=[
            vm((rows, full), BF),
            vm((full, pairs * TRIO), BF),
            vm((full, rows), BF),
            vm((deep * feat, group * rows), BF),
            vm((pairs, max(deep * feat, rows), TRIO), F32),
            vm((pairs, rows, LANES), BF),
            vm((pairs, ext, LANES), BF),
            vm((pairs, ext, LANES), BF),
            vm((pairs, rows, LANES), BF),
            vm((2 * pairs, 1, LINE), F32),
            vm((2 * pairs, 1, LINE), F32),
            vm((KB, 2 * QB), F32),
            vm((KB, 2 * QB), F32),
            vm((2, ext, LANES), F32),
            vm((2, ext, LANES), F32),
            vm((pairs, 2, HALO, LANES), BF),
            vm((pairs, 2, HALO, LANES), BF),
            vm((pairs, group * rows, LANES), BF),
            vm((pairs, group * rows, 2 * LANES), BF),
            vm((pairs, deep, feat, LANES), BF),
            vm((pairs, deep, feat, 2 * LANES), BF),
            vm((pairs, deep, feat, LANES), BF),
            vm((pairs, deep, feat, 2 * LANES), BF),
            vm(((tps - 1) * tiles, rows, TILE), BF),
            vm(((tps - 1) * tiles, rows, TILE), BF),
            vm((group, 2 * pairs, LINE), F32),
            vm((deep, 2 * pairs, LINE), F32),
            vm((tps - 1, CHUNK, dloc), BF),
            vm((rows, dloc), BF),
            vm((3, feat, width), F32),
            vm((heads, rel_bias.shape[0]), F32),
            dma((3,)),
            dma(()), dma(()), dma(()),
            dma((tps - 1, chunks)), dma((tps - 1, chunks)),
            dma((3,)), dma((3,)), dma((2,)),
            dma((2,)), dma((2,)),
            dma(()), dma((pairs,)),
            dma((2, wide - 1)), dma((2, pairs, wide - 1)),
            dma((2, wide)), dma((2, pairs, wide)),
            dma((2,)), dma((2, pairs, deep - 1)),
            dma((2,)), dma((2, pairs, deep - 1)),
            dma((2,)), dma((2,)),
            dma(()), dma(()),
        ],
        compiler_params=pltpu.CompilerParams(
            collective_id=0, has_side_effects=True, vmem_limit_bytes=67043328
        ),
        name="whole_step",
    )(inputs, w_query, w_key, w_value, rel_bias.T, d_out)
    grad = sds((feat, width), F32)
    out = pl.pallas_call(
        hand_body,
        in_specs=[hbm] * 3,
        out_specs=[hbm] * 5,
        out_shape=[sds((rows, dloc), BF), grad, grad, grad, sds((heads, rel_bias.shape[0]), F32)],
        scratch_shapes=[
            vm((rows, dloc), BF), vm((3, feat, width), F32), vm((heads, rel_bias.shape[0]), F32),
            dma((6,)), dma((6,)),
        ],
        name="hand_out",
    )(*out)
    return out[0], out[1], out[2], out[3], out[4].T


def solution(mesh):
    placed = (
        P("sp", "tp"),
        P(None, "tp"),
        P(None, "tp"),
        P(None, "tp"),
        P(None, "tp"),
        P("sp", "tp"),
    )
    sizes = (mesh.shape["sp"], mesh.shape["tp"])
    return jax.shard_map(
        functools.partial(local, sizes),
        mesh=mesh,
        in_specs=placed,
        out_specs=(P("sp", "tp"), P("sp", "tp"), P("sp", "tp"), P("sp", "tp"), P(None, "tp")),
        check_vma=False,
    )
```
